256 devices in a mesh: sp: 64 (over z, y, core), tp: 4 (over x).
Axes of the slice: x: 4, y: 4, z: 8, core: 2. Of those that a mesh axis runs over, the one named last changes fastest.
Arguments:
- resid: bfloat16 [12288, 2048], P('sp'), may hold values from -6 to 6
- query_broad: bfloat16 [12288, 1536], P('sp', 'tp'), may hold values from -60 to 60
- query_narrow: bfloat16 [12288, 1024], P('sp', 'tp'), may hold values from -60 to 60
- latent: bfloat16 [12288, 512], P('sp'), may hold values from -6 to 6
- key_rope: bfloat16 [12288, 64], P('sp'), may hold values from -6 to 6
- latent_gain: float32 [512], replicated, may hold values from 0.1 to 1.9
- key_up_broad: bfloat16 [512, 1024], P(None, 'tp'), may hold values from -0.25 to 0.25
- value_up_broad: bfloat16 [512, 1024], P(None, 'tp'), may hold values from -0.25 to 0.25
- key_up_narrow: bfloat16 [512, 512], P(None, 'tp'), may hold values from -0.25 to 0.25
- value_up_narrow: bfloat16 [512, 512], P(None, 'tp'), may hold values from -0.25 to 0.25
- out_broad: bfloat16 [1024, 2048], replicated, may hold values from -0.15625 to 0.15625
- out_narrow: bfloat16 [512, 2048], replicated, may hold values from -0.15625 to 0.15625
- post_gain: float32 [2048], replicated, may hold values from 0.1 to 1.9
- ffn_gain: float32 [2048], replicated, may hold values from 0.1 to 1.9
- up_weight: bfloat16 [2048, 8192], P('sp', 'tp'), may hold values from -0.125 to 0.125
- down_weight: bfloat16 [2048, 8192], P('sp', 'tp'), may hold values from -0.0625 to 0.0625
- ffn_out_gain: float32 [2048], replicated, may hold values from 0.1 to 1.9
Outputs:
- layer_out: bfloat16 [12288, 2048], P(('sp', 'tp'))
The draws below stay inside these ranges and needn't reach their ends.
All inputs are finite; a program needn't handle non-finite values.
Results may differ from the reference program's by a relative error of at most 0.013.
Values may be sent and summed in bfloat16 or wider, within the bound.
No kernel may reach another device: no remote copies, remote signals or barrier semaphores. Data moves between devices by JAX's collectives and lax.ppermute only.
A program may use at most 128 MiB of HBM per device.

```python
import math
import jax
import jax.numpy as jnp
from jax import lax

D = 2048
FF = 8192
R = 512
ROPE = 64
DB = 128
DN = 64
HB = 8
HN = 8
SEQ = 12288


def drawn_queries(key, salt, head_count, head_size):
    drawn = jax.random.normal(jax.random.fold_in(key, salt), (SEQ, head_count, head_size + ROPE), jnp.float32)
    return jnp.clip(drawn, -6.0, 6.0)


def draw_query_broad(key, part):
    entries = drawn_queries(key, 21, HB, DB)
    return entries.reshape(SEQ, HB * (DB + ROPE)).astype(jnp.bfloat16)


def draw_query_narrow(key, part):
    entries = drawn_queries(key, 31, HN, DN)
    return entries.reshape(SEQ, HN * (DN + ROPE)).astype(jnp.bfloat16)


def draw_key_rope(key, part):
    entries = jnp.clip(jax.random.normal(jax.random.fold_in(key, 11), (SEQ, ROPE), jnp.float32), -6.0, 6.0)
    return entries.astype(jnp.bfloat16)


def block_scale(rng, dims, cuts, least, top_value):
    def one(dim, shards_of):
        heights = jax.random.uniform(jax.random.fold_in(jax.random.fold_in(rng, 6), dim), (shards_of,), jnp.float32, least / len(cuts), top_value / len(cuts))
        return jnp.repeat(jnp.exp(heights), dims[dim] // shards_of).reshape((-1,) + (1,) * (len(dims) - dim - 1))

    factor_of = one(*cuts[0])
    for cut in cuts[1:]:
        factor_of = factor_of * one(*cut)
    return factor_of


def bell_draw(rng, extent, width, reach, cuts=(), held_as=jnp.bfloat16):
    factor_of = block_scale(rng, extent, cuts, -0.22, 0.18) if cuts else 1.0
    result = jax.random.normal(rng, extent, jnp.float32) * width * factor_of
    return jnp.minimum(jnp.maximum(result, -reach), reach).astype(held_as)


def setup_inputs(seed: int = 0) -> dict:
    streams_of = jax.random.split(jax.random.key(seed), 18)
    return {
        "resid": bell_draw(streams_of[0], (SEQ, D), 1.0, 6.0, ((0, 64),)),
        "query_broad": draw_query_broad(jax.random.fold_in(streams_of[17], 71), 0),
        "query_narrow": draw_query_narrow(jax.random.fold_in(streams_of[17], 71), 0),
        "latent": bell_draw(streams_of[3], (SEQ, R), 1.0, 6.0, ((0, 64),)),
        "key_rope": draw_key_rope(jax.random.fold_in(streams_of[17], 71), 0),
        "latent_gain": jnp.clip(1.0 + 0.18 * jax.random.normal(streams_of[5], (R,), jnp.float32), 0.1, 1.9),
        "key_up_broad": bell_draw(streams_of[6], (R, HB * DB), R ** -0.5, 0.25, ((1, 4),)),
        "value_up_broad": bell_draw(streams_of[7], (R, HB * DB), R ** -0.5, 0.25, ((1, 4),)),
        "key_up_narrow": bell_draw(streams_of[8], (R, HN * DN), R ** -0.5, 0.25, ((1, 4),)),
        "value_up_narrow": bell_draw(streams_of[9], (R, HN * DN), R ** -0.5, 0.25, ((1, 4),)),
        "out_broad": bell_draw(streams_of[10], (HB * DB, D), (HB * DB + HN * DN) ** -0.5, 0.15625),
        "out_narrow": bell_draw(streams_of[11], (HN * DN, D), (HB * DB + HN * DN) ** -0.5, 0.15625),
        "post_gain": jnp.clip(1.0 + 0.18 * jax.random.normal(streams_of[12], (D,), jnp.float32), 0.1, 1.9),
        "ffn_gain": jnp.clip(1.0 + 0.18 * jax.random.normal(streams_of[13], (D,), jnp.float32), 0.1, 1.9),
        "up_weight": bell_draw(streams_of[14], (D, FF), D ** -0.5, 0.125, ((0, 64), (1, 4))),
        "down_weight": bell_draw(streams_of[15], (D, FF), FF ** -0.5, 0.0625, ((0, 64), (1, 4))),
        "ffn_out_gain": jnp.clip(1.0 + 0.18 * jax.random.normal(streams_of[16], (D,), jnp.float32), 0.1, 1.9),
    }


norm_eps = 1e-06
rope_base = 500000.0
masked_score = -1e+30

def rotate(values, positions):
    full_width = values.shape[-1]
    half_width = full_width // 2
    frequency = rope_base ** (-2.0 * jnp.arange(half_width, dtype=jnp.float32) / full_width)
    angles = positions.astype(jnp.float32)[:, None] * frequency[None, :]
    angle_shape = (angles.shape[0],) + (1,) * (values.ndim - 2) + (half_width,)
    cosine = jnp.cos(angles).reshape(angle_shape)
    sine_part = jnp.sin(angles).reshape(angle_shape)
    leading = values[..., :half_width]
    trailing = values[..., half_width:]
    return jnp.concatenate([leading * cosine - trailing * sine_part, trailing * cosine + leading * sine_part], axis=-1)

def rms_scale(values, norm_gain):
    return values * lax.rsqrt(lax.optimization_barrier(jnp.mean(values * values, axis=-1, keepdims=True)) + norm_eps) * norm_gain

def attend_all(query_nope, query_rope, key_rows, key_rot, value_rows, score_scale):
    block_rows = math.gcd(SEQ, 512)
    positions = jnp.arange(SEQ, dtype=jnp.int32)
    keys_wide = key_rows.astype(jnp.float32)
    rot_wide = key_rot.astype(jnp.float32)
    values_wide = value_rows.astype(jnp.float32)

    def one_block(block_index):
        begin = block_index * block_rows
        nope_part = lax.dynamic_slice_in_dim(query_nope, begin, block_rows, 0).astype(jnp.float32)
        rope_part = lax.dynamic_slice_in_dim(query_rope, begin, block_rows, 0).astype(jnp.float32)
        query_pos = begin + jnp.arange(block_rows, dtype=jnp.int32)
        scores = jnp.einsum('qhd,khd->hqk', nope_part, keys_wide) + jnp.einsum('qhd,kd->hqk', rope_part, rot_wide)
        scores = scores * score_scale
        allowed = (positions[None, :] <= query_pos[:, None])[None]
        scores = jnp.where(allowed, scores, masked_score)
        highest = lax.optimization_barrier(jnp.max(scores, axis=-1, keepdims=True))
        exponent = jnp.where(allowed, jnp.exp(scores - highest), 0.0)
        denominator = lax.optimization_barrier(jnp.sum(exponent, axis=-1))
        rounded = lax.optimization_barrier(exponent.astype(jnp.bfloat16)).astype(jnp.float32)
        summed = jnp.einsum('hqk,khd->qhd', rounded, values_wide)
        return (summed / jnp.transpose(denominator)[:, :, None]).astype(jnp.bfloat16)
    heads_out = lax.map(one_block, jnp.arange(SEQ // block_rows, dtype=jnp.int32))
    return heads_out.reshape(SEQ, value_rows.shape[1] * value_rows.shape[2])

def reference(resid, query_broad, query_narrow, latent, key_rope, latent_gain, key_up_broad, value_up_broad, key_up_narrow, value_up_narrow, out_broad, out_narrow, post_gain, ffn_gain, up_weight, down_weight, ffn_out_gain):
    positions = jnp.arange(SEQ, dtype=jnp.int32)
    latent_normed = rms_scale(latent.astype(jnp.float32), latent_gain).astype(jnp.bfloat16)

    def expand(weight, head_size):
        product = jnp.dot(latent_normed, weight, preferred_element_type=jnp.float32)
        return product.astype(jnp.bfloat16).reshape(SEQ, -1, head_size)
    key_broad = expand(key_up_broad, DB)
    value_broad = expand(value_up_broad, DB)
    key_narrow = expand(key_up_narrow, DN)
    value_narrow = expand(value_up_narrow, DN)
    key_rot = rotate(key_rope.astype(jnp.float32), positions).astype(jnp.bfloat16)
    broad_heads = query_broad.reshape(SEQ, HB, DB + ROPE)
    broad_rope = rotate(broad_heads[:, :, DB:].astype(jnp.float32), positions).astype(jnp.bfloat16)
    narrow_heads = query_narrow.reshape(SEQ, HN, DN + ROPE)
    narrow_rope = rotate(narrow_heads[:, :, DN:].astype(jnp.float32), positions).astype(jnp.bfloat16)
    attn_broad = attend_all(broad_heads[:, :, :DB], broad_rope, key_broad, key_rot, value_broad, (DB + ROPE) ** (-0.5))
    attn_narrow = attend_all(narrow_heads[:, :, :DN], narrow_rope, key_narrow, key_rot, value_narrow, (DN + ROPE) ** (-0.5))
    projected = jnp.dot(attn_broad, out_broad, preferred_element_type=jnp.float32) + jnp.dot(attn_narrow, out_narrow, preferred_element_type=jnp.float32)
    mixed = (resid.astype(jnp.float32) + rms_scale(projected, post_gain)).astype(jnp.bfloat16)
    normed = rms_scale(mixed.astype(jnp.float32), ffn_gain).astype(jnp.bfloat16)
    hidden = jnp.square(jax.nn.relu(jnp.dot(normed, up_weight, preferred_element_type=jnp.float32))).astype(jnp.bfloat16)
    ffn = lax.dot_general(hidden, down_weight, (((1,), (1,)), ((), ())), preferred_element_type=jnp.float32)
    return (mixed.astype(jnp.float32) + rms_scale(ffn, ffn_out_gain)).astype(jnp.bfloat16)
```

```python
import functools
import math

import jax
import jax.numpy as jnp
from jax import lax
from jax.experimental import pallas as pl
from jax.experimental.pallas import tpu as pltpu
from jax.sharding import Mesh, PartitionSpec as P

NZ, NY, NC = 8, 4, 2
DB, DN, ROPE, R = 128, 64, 64, 512
norm_eps = 1e-06
rope_base = 500000.0
low = -1e30
LOG2E = math.log2(math.e)
SP = ("z", "y", "c")


def rms_scale(values, norm_gain):
    return (
        values * lax.rsqrt(jnp.mean(values * values, axis=-1, keepdims=True) + norm_eps) * norm_gain
    )


def shift(value, axis, by):
    size = lax.axis_size(axis)
    return lax.ppermute(value, axis, [(i, (i + by) % size) for i in range(size)])


def ring(own, axis):
    size, rows = lax.axis_size(axis), own.shape[0]
    half = size // 2
    up, down = [own], [own]
    for _ in range(half - 1):
        up.append(shift(up[-1], axis, 1))
        down.append(shift(down[-1], axis, -1))
    far = [
        shift(up[-1][: rows // 2], axis, 1),
        shift(down[-1][rows // 2 :], axis, -1),
    ]
    return jnp.concatenate(up + far + down[:0:-1], axis=0)


def attention_kernel(
    where_ref, q_ref, mine_ref, other_ref, wk_ref, wvt_ref, cos_ref, sin_ref, out_ref,
    qt_ref, kc_ref, vt_ref, acc_ref, m_ref, l_ref, *, rows,
):
    f32, bf16 = jnp.float32, jnp.bfloat16
    z, y, c = where_ref[0], where_ref[1], where_ref[2]
    nq, pair = NY * rows, 2 * rows
    nk = 2 * pair
    tile = 256

    qt = q_ref[...].astype(f32).T
    cosine, sine = cos_ref[...], sin_ref[...]

    def rotated(at):
        a, b = qt[at : at + 32], qt[at + 32 : at + 64]
        return (a * cosine - b * sine).astype(bf16), (b * cosine + a * sine).astype(bf16)

    zeros = jnp.zeros((64, nq), bf16)
    for h in range(4):
        if h < 2:
            at = h * (DB + ROPE)
            qt_ref[h, 0:128] = qt[at : at + DB].astype(bf16)
            first, second = rotated(at + DB)
        else:
            at = 2 * (DB + ROPE) + (h - 2) * (DN + ROPE)
            mine, others = (h - 2) * 64, (3 - h) * 64
            qt_ref[h, mine : mine + 64] = qt[at : at + DN].astype(bf16)
            qt_ref[h, others : others + 64] = zeros
            first, second = rotated(at + DN)
        qt_ref[h, 128:160] = first
        qt_ref[h, 160:192] = second
        qt_ref[h, 192:256] = zeros

    acc_ref[...] = jnp.zeros_like(acc_ref)
    l_ref[...] = jnp.zeros_like(l_ref)
    m_ref[...] = jnp.full_like(m_ref, low)

    def step(p, masked):
        at = pl.multiple_of(p * pair, pair)
        chunk = jnp.concatenate(
            [mine_ref[pl.ds(at, pair), :], other_ref[pl.ds(at, pair), :]], axis=0
        )
        normed, rope = chunk[:, :R], chunk[:, R:]
        keys = jnp.dot(normed, wk_ref[...], preferred_element_type=f32).astype(bf16)
        for k in range(3):
            kc_ref[k, :, 0:128] = keys[:, 128 * k : 128 * (k + 1)]
            kc_ref[k, :, 128:256] = rope
        vt_ref[...] = lax.dot_general(
            wvt_ref[...], normed, (((1,), (1,)), ((), ())), preferred_element_type=f32
        ).astype(bf16)
        if masked:
            row = lax.broadcasted_iota(jnp.int32, (nk, 1), 0)
            second = (row >= pair).astype(jnp.int32)
            row = row - second * pair
            later = (row >= rows).astype(jnp.int32)
            row = row - later * rows
            core = c + second * (1 - 2 * c)
            zk = z - 2 * p - later
            zk = jnp.where(zk < 0, zk + NZ, zk)
            key_pos = ((zk * NY + y) * NC + core) * rows + row

        def q_tile(t, carry):
            lanes = pl.ds(pl.multiple_of(t * tile, tile), tile)
            if masked:
                col = lax.broadcasted_iota(jnp.int32, (1, tile), 1) + t * tile
                block = (col >= rows).astype(jnp.int32)
                block += (col >= 2 * rows).astype(jnp.int32)
                block += (col >= 3 * rows).astype(jnp.int32)
                yq = y - block
                yq = jnp.where(yq < 0, yq + NY, yq)
                q_pos = ((z * NY + yq) * NC + c) * rows + col - block * rows
                allowed = key_pos <= q_pos
            for h in range(4):
                scale = LOG2E * ((DB if h < 2 else DN) + ROPE) ** (-0.5)
                s = jnp.dot(
                    kc_ref[min(h, 2)], qt_ref[h, :, lanes], preferred_element_type=f32
                )
                s = s * scale
                if masked:
                    s = jnp.where(allowed, s, low)
                old = m_ref[h : h + 1, lanes]
                new = jnp.maximum(old, jnp.max(s, axis=0, keepdims=True))
                weight = jnp.exp2(s - new)
                if masked:
                    weight = jnp.where(allowed, weight, 0.0)
                factor = jnp.exp2(old - new)
                m_ref[h : h + 1, lanes] = new
                l_ref[h : h + 1, lanes] = l_ref[h : h + 1, lanes] * factor + jnp.sum(
                    weight, axis=0, keepdims=True
                )
                dims = slice(h * 128, h * 128 + 128) if h < 2 else slice(128 + h * 64, 192 + h * 64)
                acc_ref[dims, lanes] = acc_ref[dims, lanes] * factor + jnp.dot(
                    vt_ref[dims, :], weight.astype(bf16), preferred_element_type=f32
                )
            return carry

        lax.fori_loop(0, nq // tile, q_tile, 0)

    def one(p, carry):
        clear = jnp.logical_and(p > 0, 2 * p + 1 <= z)

        @pl.when(clear)
        def _():
            step(p, False)

        @pl.when(jnp.logical_not(clear))
        def _():
            step(p, True)

        return carry

    lax.fori_loop(0, lax.div(z, 2) + 1, one, 0)

    total = l_ref[...]
    some = total > 0.0
    inverse = jnp.where(some, 1.0 / jnp.where(some, total, 1.0), 0.0)
    lse = jnp.where(some, m_ref[...] + jnp.log2(jnp.where(some, total, 1.0)), low)
    high = lse.astype(bf16).astype(f32)
    middle = (lse - high).astype(bf16).astype(f32)
    last = lse - high - middle
    parts = [
        acc_ref[0:128] * inverse[0:1],
        acc_ref[128:256] * inverse[1:2],
        acc_ref[256:320] * inverse[2:3],
        acc_ref[320:384] * inverse[3:4],
        high,
        middle,
        last,
        jnp.zeros((104, nq), f32),
    ]
    packed = jnp.concatenate(parts, axis=0).T.astype(bf16)
    for e in range(NY):
        yq = y - e
        yq = jnp.where(yq < 0, yq + NY, yq)
        out_ref[pl.ds(pl.multiple_of(yq * rows, rows), rows), :] = packed[e * rows : (e + 1) * rows]


def attention(where, q, mine, other, wk, wvt, cosine, sine, rows):
    nq, nk = NY * rows, 4 * rows
    vmem = pl.BlockSpec(memory_space=pltpu.VMEM)
    return pl.pallas_call(
        functools.partial(attention_kernel, rows=rows),
        out_shape=jax.ShapeDtypeStruct((nq, 512), jnp.bfloat16),
        in_specs=[pl.BlockSpec(memory_space=pltpu.SMEM)] + [vmem] * 7,
        out_specs=vmem,
        scratch_shapes=[
            pltpu.VMEM((4, 256, nq), jnp.bfloat16),
            pltpu.VMEM((3, nk, 256), jnp.bfloat16),
            pltpu.VMEM((384, nk), jnp.bfloat16),
            pltpu.VMEM((384, nq), jnp.float32),
            pltpu.VMEM((8, nq), jnp.float32),
            pltpu.VMEM((8, nq), jnp.float32),
        ],
        compiler_params=pltpu.CompilerParams(vmem_limit_bytes=48 * 1024 * 1024),
        cost_estimate=pl.CostEstimate(
            flops=20_000_000_000, bytes_accessed=8_000_000, transcendentals=10_000_000
        ),
        name="attention",
    )(where, q, mine, other, wk, wvt, cosine, sine)


def combine_kernel(part_ref, out_ref):
    f32 = jnp.float32
    stats = []
    for s in range(NY):
        st = part_ref[s, :, 384:512].astype(f32)
        stats.append(st + pltpu.roll(st, 120, 1) + pltpu.roll(st, 112, 1))
    top = functools.reduce(jnp.maximum, stats)
    weights = [jnp.exp2(st - top) for st in stats]
    inverse = 1.0 / functools.reduce(jnp.add, weights)
    weights = [w * inverse for w in weights]
    lane = lax.broadcasted_iota(jnp.int32, (1, 128), 1)
    for k in range(3):
        total = None
        for s in range(NY):
            w = weights[s]
            if k < 2:
                factor = w[:, k : k + 1]
            else:
                factor = jnp.where(lane < 64, w[:, 2:3], w[:, 3:4])
            term = part_ref[s, :, 128 * k : 128 * (k + 1)].astype(f32) * factor
            total = term if total is None else total + term
        out_ref[:, 128 * k : 128 * (k + 1)] = total.astype(jnp.bfloat16)


def combine(parts):
    vmem = pl.BlockSpec(memory_space=pltpu.VMEM)
    return pl.pallas_call(
        combine_kernel,
        out_shape=jax.ShapeDtypeStruct((parts.shape[1], 384), jnp.bfloat16),
        in_specs=[vmem],
        out_specs=vmem,
        cost_estimate=pl.CostEstimate(flops=1_000_000, bytes_accessed=1_000_000, transcendentals=0),
        name="combine",
    )(parts)


def angles(positions):
    frequency = rope_base ** (-2.0 * jnp.arange(ROPE // 2, dtype=jnp.float32) / ROPE)
    return positions.astype(jnp.float32), frequency


def local(
    resid, query_broad, query_narrow, latent, key_rope, latent_gain, key_up_broad, value_up_broad,
    key_up_narrow, value_up_narrow, out_broad, out_narrow, post_gain, ffn_gain, up_weight,
    down_weight, ffn_out_gain,
):
    f32, bf16 = jnp.float32, jnp.bfloat16
    rows = resid.shape[0]
    z, y, c = (lax.axis_index(a) for a in SP)
    first = ((z * NY + y) * NC + c) * rows
    within = jnp.arange(rows, dtype=jnp.int32)

    both = lax.all_gather(
        jnp.concatenate([up_weight, down_weight], axis=1), SP, axis=0, tiled=True
    )

    normed_latent = rms_scale(latent.astype(f32), latent_gain).astype(bf16)
    pos, frequency = angles(first + within)
    angle = pos[:, None] * frequency[None, :]
    ka, kb = key_rope[:, :32].astype(f32), key_rope[:, 32:].astype(f32)
    cosine, sine = jnp.cos(angle), jnp.sin(angle)
    key_rot = jnp.concatenate([ka * cosine - kb * sine, kb * cosine + ka * sine], axis=1)
    sent = jnp.concatenate(
        [normed_latent, key_rot.astype(bf16), jnp.zeros((rows, 64), bf16)], axis=1
    )
    mine = ring(sent, "z")
    other = lax.ppermute(mine, "c", [(0, 1), (1, 0)])
    queries = ring(jnp.concatenate([query_broad, query_narrow], axis=1), "y")

    block_y = jnp.mod(y - jnp.arange(NY, dtype=jnp.int32), NY)
    q_pos = ((z * NY + block_y) * NC + c)[:, None] * rows + within[None, :]
    pos, frequency = angles(q_pos.reshape(-1))
    angle = frequency[:, None] * pos[None, :]
    wk = jnp.concatenate([key_up_broad, key_up_narrow], axis=1)
    wvt = jnp.concatenate([value_up_broad, value_up_narrow], axis=1).T
    where = jnp.stack([z, y, c]).astype(jnp.int32)
    partial = attention(
        where, queries, mine, other, wk, wvt, jnp.cos(angle), jnp.sin(angle), rows
    )
    parts = lax.all_to_all(partial.reshape(NY, rows, 512), "y", 0, 0, tiled=True)
    attn = combine(parts)
    heads = lax.all_gather(attn, "x", axis=0)
    nx = heads.shape[0]
    attn_broad = jnp.moveaxis(heads[:, :, :256], 0, 1).reshape(rows, nx * 256)
    attn_narrow = jnp.moveaxis(heads[:, :, 256:], 0, 1).reshape(rows, nx * 128)
    projected = jnp.dot(attn_broad, out_broad, preferred_element_type=f32) + jnp.dot(
        attn_narrow, out_narrow, preferred_element_type=f32
    )
    mixed = (resid.astype(f32) + rms_scale(projected, post_gain)).astype(bf16)
    normed = rms_scale(mixed.astype(f32), ffn_gain).astype(bf16)
    units = up_weight.shape[1]
    hidden = jnp.square(
        jax.nn.relu(jnp.dot(normed, both[:, :units], preferred_element_type=f32))
    ).astype(bf16)
    share = lax.dot_general(
        hidden, both[:, units:], (((1,), (1,)), ((), ())), preferred_element_type=f32
    ).astype(bf16)
    own_rows = rows // nx
    shares = lax.all_to_all(share.reshape(nx, own_rows, -1), "x", 0, 0, tiled=True)
    ffn = jnp.sum(shares.astype(f32), axis=0)
    own = lax.dynamic_slice_in_dim(mixed, lax.axis_index("x") * own_rows, own_rows, 0)
    return (own.astype(f32) + rms_scale(ffn, ffn_out_gain)).astype(bf16)


def solution(mesh):
    grid = Mesh(mesh.devices.reshape(NZ, NY, NC, -1), ("z", "y", "c", "x"))
    row, split, heads = P(SP, None), P(SP, "x"), P(None, "x")
    in_specs = (
        row, split, split, row, row, P(), heads, heads, heads, heads, P(), P(), P(), P(),
        split, split, P(),
    )
    return jax.shard_map(
        local, mesh=grid, in_specs=in_specs, out_specs=P(("z", "y", "c", "x"), None), check_vma=False
    )
```

```python
import functools
import math

import jax
import jax.numpy as jnp
from jax import lax
from jax.experimental import pallas as pl
from jax.experimental.pallas import tpu as pltpu
from jax.sharding import Mesh, PartitionSpec as P

NZ, NY, NC = 8, 4, 2
DB, DN, ROPE, R = 128, 64, 64, 512
norm_eps = 1e-06
rope_base = 500000.0
low = -1e30
LOG2E = math.log2(math.e)
SP = ("z", "y", "c")


def rms_scale(values, norm_gain):
    return (
        values * lax.rsqrt(jnp.mean(values * values, axis=-1, keepdims=True) + norm_eps) * norm_gain
    )


def shift(value, axis, by):
    size = lax.axis_size(axis)
    return lax.ppermute(value, axis, [(i, (i + by) % size) for i in range(size)])


def across(value):
    return lax.ppermute(value, "c", [(0, 1), (1, 0)])


def gathered(own, queries):
    half = own.shape[0] // 2
    stage = lax.optimization_barrier
    up1, down1, q1, q3, o0 = stage(
        (
            shift(own, "z", 1),
            shift(own, "z", -1),
            shift(queries, "y", 1),
            shift(queries, "y", -1),
            across(own),
        )
    )
    up2, down2, q2a, q2b, o1, o7 = stage(
        (
            shift(up1, "z", 1),
            shift(down1, "z", -1),
            shift(q1[:half], "y", 1),
            shift(q3[half:], "y", -1),
            across(up1),
            across(down1),
        )
    )
    up3, down3, o2, o6 = stage(
        (shift(up2, "z", 1), shift(down2, "z", -1), across(up2), across(down2))
    )
    far_a, far_b, o3, o5 = stage(
        (
            shift(up3[:half], "z", 1),
            shift(down3[half:], "z", -1),
            across(up3),
            across(down3),
        )
    )
    mine = (own, up1, up2, up3, far_a, far_b, down3, down2, down1)
    other = (o0, o1, o2, o3, across(far_a), across(far_b), o5, o6, o7)
    return (queries, q1, q2a, q2b, q3), mine, other


def attention_kernel(
    where_ref, *refs, rows
):
    q_refs, mine_refs, other_refs = refs[:5], refs[5:14], refs[14:23]
    wk_ref, wvt_ref, cos_ref, sin_ref, out_ref = refs[23:28]
    lat_ref, qt_ref, kc_ref, vt_ref, acc_ref, m_ref, l_ref = refs[28:]
    f32, bf16 = jnp.float32, jnp.bfloat16
    z, y, c = where_ref[0], where_ref[1], where_ref[2]
    nq, pair = NY * rows, 2 * rows
    nk = 2 * pair
    tile = 256

    qt = jnp.concatenate([r[...] for r in q_refs], axis=0).astype(f32).T
    cosine, sine = cos_ref[...], sin_ref[...]

    def rotated(at):
        a, b = qt[at : at + 32], qt[at + 32 : at + 64]
        return (a * cosine - b * sine).astype(bf16), (b * cosine + a * sine).astype(bf16)

    zeros = jnp.zeros((64, nq), bf16)
    for h in range(4):
        if h < 2:
            at = h * (DB + ROPE)
            qt_ref[h, 0:128] = qt[at : at + DB].astype(bf16)
            first, second = rotated(at + DB)
        else:
            at = 2 * (DB + ROPE) + (h - 2) * (DN + ROPE)
            mine, others = (h - 2) * 64, (3 - h) * 64
            qt_ref[h, mine : mine + 64] = qt[at : at + DN].astype(bf16)
            qt_ref[h, others : others + 64] = zeros
            first, second = rotated(at + DN)
        qt_ref[h, 128:160] = first
        qt_ref[h, 160:192] = second
        qt_ref[h, 192:256] = zeros

    for side, pieces in enumerate((mine_refs, other_refs)):
        at = 0
        for r in pieces:
            lat_ref[side, at : at + r.shape[0], :] = r[...]
            at += r.shape[0]

    acc_ref[...] = jnp.zeros_like(acc_ref)
    l_ref[...] = jnp.zeros_like(l_ref)
    m_ref[...] = jnp.full_like(m_ref, low)

    def step(p, masked):
        at = pl.multiple_of(p * pair, pair)
        chunk = jnp.concatenate(
            [lat_ref[0, pl.ds(at, pair), :], lat_ref[1, pl.ds(at, pair), :]], axis=0
        )
        normed, rope = chunk[:, :R], chunk[:, R:]
        keys = jnp.dot(normed, wk_ref[...], preferred_element_type=f32).astype(bf16)
        for k in range(3):
            kc_ref[k, :, 0:128] = keys[:, 128 * k : 128 * (k + 1)]
            kc_ref[k, :, 128:256] = rope
        vt_ref[...] = lax.dot_general(
            wvt_ref[...], normed, (((1,), (1,)), ((), ())), preferred_element_type=f32
        ).astype(bf16)
        if masked:
            row = lax.broadcasted_iota(jnp.int32, (nk, 1), 0)
            second = (row >= pair).astype(jnp.int32)
            row = row - second * pair
            later = (row >= rows).astype(jnp.int32)
            row = row - later * rows
            core = c + second * (1 - 2 * c)
            zk = z - 2 * p - later
            zk = jnp.where(zk < 0, zk + NZ, zk)
            key_pos = ((zk * NY + y) * NC + core) * rows + row

        def q_tile(t, carry):
            lanes = pl.ds(pl.multiple_of(t * tile, tile), tile)
            if masked:
                col = lax.broadcasted_iota(jnp.int32, (1, tile), 1) + t * tile
                block = (col >= rows).astype(jnp.int32)
                block += (col >= 2 * rows).astype(jnp.int32)
                block += (col >= 3 * rows).astype(jnp.int32)
                yq = y - block
                yq = jnp.where(yq < 0, yq + NY, yq)
                q_pos = ((z * NY + yq) * NC + c) * rows + col - block * rows
                allowed = key_pos <= q_pos
            def scores(h):
                return jnp.dot(
                    kc_ref[min(h, 2)], qt_ref[h, :, lanes], preferred_element_type=f32
                )

            ahead = scores(0)
            for h in range(4):
                scale = LOG2E * ((DB if h < 2 else DN) + ROPE) ** (-0.5)
                s = ahead
                if h < 3:
                    ahead = scores(h + 1)
                if masked:
                    s = jnp.where(allowed, s, low)
                old = m_ref[h : h + 1, lanes]
                new = jnp.maximum(old, jnp.max(s, axis=0, keepdims=True))
                weight = jnp.exp2((s - new) * scale)
                if masked:
                    weight = jnp.where(allowed, weight, 0.0)
                factor = jnp.exp2((old - new) * scale)
                m_ref[h : h + 1, lanes] = new
                l_ref[h : h + 1, lanes] = l_ref[h : h + 1, lanes] * factor + jnp.sum(
                    weight, axis=0, keepdims=True
                )
                dims = slice(h * 128, h * 128 + 128) if h < 2 else slice(128 + h * 64, 192 + h * 64)
                acc_ref[dims, lanes] = acc_ref[dims, lanes] * factor + jnp.dot(
                    vt_ref[dims, :], weight.astype(bf16), preferred_element_type=f32
                )
            return carry

        lax.fori_loop(0, nq // tile, q_tile, 0)

    def one(p, carry):
        clear = jnp.logical_and(p > 0, 2 * p + 1 <= z)

        @pl.when(clear)
        def _():
            step(p, False)

        @pl.when(jnp.logical_not(clear))
        def _():
            step(p, True)

        return carry

    lax.fori_loop(0, lax.div(z, 2) + 1, one, 0)

    total = l_ref[...]
    some = total > 0.0
    inverse = jnp.where(some, 1.0 / jnp.where(some, total, 1.0), 0.0)
    head = lax.broadcasted_iota(jnp.int32, (8, 1), 0)
    scale = jnp.where(head < 2, LOG2E * (DB + ROPE) ** (-0.5), LOG2E * (DN + ROPE) ** (-0.5))
    lse = jnp.where(some, m_ref[...] * scale + jnp.log2(jnp.where(some, total, 1.0)), low)
    high = lse.astype(bf16).astype(f32)
    middle = (lse - high).astype(bf16).astype(f32)
    last = lse - high - middle
    parts = [
        acc_ref[0:128] * inverse[0:1],
        acc_ref[128:256] * inverse[1:2],
        acc_ref[256:320] * inverse[2:3],
        acc_ref[320:384] * inverse[3:4],
        high,
        middle,
        last,
        jnp.zeros((104, nq), f32),
    ]
    packed = jnp.concatenate(parts, axis=0).T.astype(bf16)
    for e in range(NY):
        yq = y - e
        yq = jnp.where(yq < 0, yq + NY, yq)
        out_ref[pl.ds(pl.multiple_of(yq * rows, rows), rows), :] = packed[e * rows : (e + 1) * rows]


def attention(where, q, mine, other, wk, wvt, cosine, sine, rows):
    nq, nk = NY * rows, 4 * rows
    vmem = pl.BlockSpec(memory_space=pltpu.VMEM)
    operands = (*q, *mine, *other, wk, wvt, cosine, sine)
    return pl.pallas_call(
        functools.partial(attention_kernel, rows=rows),
        out_shape=jax.ShapeDtypeStruct((nq, 512), jnp.bfloat16),
        in_specs=[pl.BlockSpec(memory_space=pltpu.SMEM)] + [vmem] * len(operands),
        out_specs=vmem,
        scratch_shapes=[
            pltpu.VMEM((2, NZ * rows, 640), jnp.bfloat16),
            pltpu.VMEM((4, 256, nq), jnp.bfloat16),
            pltpu.VMEM((3, nk, 256), jnp.bfloat16),
            pltpu.VMEM((384, nk), jnp.bfloat16),
            pltpu.VMEM((384, nq), jnp.float32),
            pltpu.VMEM((8, nq), jnp.float32),
            pltpu.VMEM((8, nq), jnp.float32),
        ],
        compiler_params=pltpu.CompilerParams(
            vmem_limit_bytes=48 * 1024 * 1024
        ),
        cost_estimate=pl.CostEstimate(
            flops=20_000_000_000, bytes_accessed=8_000_000, transcendentals=10_000_000
        ),
        name="attention",
    )(where, *operands)


def combine_kernel(part_ref, out_ref):
    f32 = jnp.float32
    stats = []
    for s in range(NY):
        st = part_ref[s, :, 384:512].astype(f32)
        stats.append(st + pltpu.roll(st, 120, 1) + pltpu.roll(st, 112, 1))
    top = functools.reduce(jnp.maximum, stats)
    weights = [jnp.exp2(st - top) for st in stats]
    inverse = 1.0 / functools.reduce(jnp.add, weights)
    weights = [w * inverse for w in weights]
    lane = lax.broadcasted_iota(jnp.int32, (1, 128), 1)
    for k in range(3):
        total = None
        for s in range(NY):
            w = weights[s]
            if k < 2:
                factor = w[:, k : k + 1]
            else:
                factor = jnp.where(lane < 64, w[:, 2:3], w[:, 3:4])
            term = part_ref[s, :, 128 * k : 128 * (k + 1)].astype(f32) * factor
            total = term if total is None else total + term
        out_ref[:, 128 * k : 128 * (k + 1)] = total.astype(jnp.bfloat16)


def combine(parts):
    vmem = pl.BlockSpec(memory_space=pltpu.VMEM)
    return pl.pallas_call(
        combine_kernel,
        out_shape=jax.ShapeDtypeStruct((parts.shape[1], 384), jnp.bfloat16),
        in_specs=[vmem],
        out_specs=vmem,
        cost_estimate=pl.CostEstimate(flops=1_000_000, bytes_accessed=1_000_000, transcendentals=0),
        name="combine",
    )(parts)


def ffn_kernel(normed_ref, up_ref, down_ref, out_ref, acc_ref):
    step = pl.program_id(0)
    up = jnp.dot(normed_ref[...], up_ref[...], preferred_element_type=jnp.float32)
    hidden = jnp.square(jnp.maximum(up, 0.0)).astype(jnp.bfloat16)
    term = lax.dot_general(
        hidden, down_ref[...], (((1,), (1,)), ((), ())), preferred_element_type=jnp.float32
    )

    @pl.when(step == 0)
    def _():
        acc_ref[...] = term

    @pl.when(step > 0)
    def _():
        acc_ref[...] += term

    @pl.when(step == pl.num_programs(0) - 1)
    def _():
        out_ref[...] = acc_ref[...].astype(jnp.bfloat16)


def feed_forward(normed, both, units):
    rows, width = normed.shape
    tile = 256
    steps = units // tile
    return pl.pallas_call(
        ffn_kernel,
        grid=(steps,),
        out_shape=jax.ShapeDtypeStruct((rows, width), jnp.bfloat16),
        in_specs=[
            pl.BlockSpec((rows, width), lambda i: (0, 0)),
            pl.BlockSpec((width, tile), lambda i: (0, i)),
            pl.BlockSpec((width, tile), lambda i: (0, steps + i)),
        ],
        out_specs=pl.BlockSpec((rows, width), lambda i: (0, 0)),
        scratch_shapes=[pltpu.VMEM((rows, width), jnp.float32)],
        compiler_params=pltpu.CompilerParams(
            dimension_semantics=("arbitrary",), vmem_limit_bytes=32 * 1024 * 1024
        ),
        cost_estimate=pl.CostEstimate(
            flops=4 * rows * width * units, bytes_accessed=4 * width * units, transcendentals=0
        ),
        name="feed_forward",
    )(normed, both, both)


def angles(positions):
    frequency = rope_base ** (-2.0 * jnp.arange(ROPE // 2, dtype=jnp.float32) / ROPE)
    return positions.astype(jnp.float32), frequency


def local(
    resid, query_broad, query_narrow, latent, key_rope, latent_gain, key_up_broad, value_up_broad,
    key_up_narrow, value_up_narrow, out_broad, out_narrow, post_gain, ffn_gain, up_weight,
    down_weight, ffn_out_gain,
):
    f32, bf16 = jnp.float32, jnp.bfloat16
    rows = resid.shape[0]
    z, y, c = (lax.axis_index(a) for a in SP)
    first = ((z * NY + y) * NC + c) * rows
    within = jnp.arange(rows, dtype=jnp.int32)

    both = lax.all_gather(
        jnp.concatenate([up_weight, down_weight], axis=1), SP, axis=0, tiled=True
    )

    normed_latent = rms_scale(latent.astype(f32), latent_gain).astype(bf16)
    pos, frequency = angles(first + within)
    angle = pos[:, None] * frequency[None, :]
    ka, kb = key_rope[:, :32].astype(f32), key_rope[:, 32:].astype(f32)
    cosine, sine = jnp.cos(angle), jnp.sin(angle)
    key_rot = jnp.concatenate([ka * cosine - kb * sine, kb * cosine + ka * sine], axis=1)
    sent = jnp.concatenate(
        [normed_latent, key_rot.astype(bf16), jnp.zeros((rows, 64), bf16)], axis=1
    )
    queries, mine, other = gathered(
        sent, jnp.concatenate([query_broad, query_narrow], axis=1)
    )

    block_y = jnp.mod(y - jnp.arange(NY, dtype=jnp.int32), NY)
    q_pos = ((z * NY + block_y) * NC + c)[:, None] * rows + within[None, :]
    pos, frequency = angles(q_pos.reshape(-1))
    angle = frequency[:, None] * pos[None, :]
    wk = jnp.concatenate([key_up_broad, key_up_narrow], axis=1)
    wvt = jnp.concatenate([value_up_broad, value_up_narrow], axis=1).T
    where = jnp.stack([z, y, c]).astype(jnp.int32)
    partial = attention(
        where, queries, mine, other, wk, wvt, jnp.cos(angle), jnp.sin(angle), rows
    )
    parts = lax.all_to_all(partial.reshape(NY, rows, 512), "y", 0, 0, tiled=True)
    attn = combine(parts)
    heads = lax.all_gather(attn, "x", axis=0)
    nx = heads.shape[0]
    attn_broad = jnp.moveaxis(heads[:, :, :256], 0, 1).reshape(rows, nx * 256)
    attn_narrow = jnp.moveaxis(heads[:, :, 256:], 0, 1).reshape(rows, nx * 128)
    projected = jnp.dot(attn_broad, out_broad, preferred_element_type=f32) + jnp.dot(
        attn_narrow, out_narrow, preferred_element_type=f32
    )
    mixed = (resid.astype(f32) + rms_scale(projected, post_gain)).astype(bf16)
    normed = rms_scale(mixed.astype(f32), ffn_gain).astype(bf16)
    units = up_weight.shape[1]
    share = feed_forward(normed, both, units)
    own_rows = rows // nx
    shares = lax.all_to_all(share.reshape(nx, own_rows, -1), "x", 0, 0, tiled=True)
    ffn = jnp.sum(shares.astype(f32), axis=0)
    own = lax.dynamic_slice_in_dim(mixed, lax.axis_index("x") * own_rows, own_rows, 0)
    return (own.astype(f32) + rms_scale(ffn, ffn_out_gain)).astype(bf16)


def solution(mesh):
    grid = Mesh(mesh.devices.reshape(NZ, NY, NC, -1), ("z", "y", "c", "x"))
    row, split, heads = P(SP, None), P(SP, "x"), P(None, "x")
    in_specs = (
        row, split, split, row, row, P(), heads, heads, heads, heads, P(), P(), P(), P(),
        split, split, P(),
    )
    return jax.shard_map(
        local, mesh=grid, in_specs=in_specs, out_specs=P(("z", "y", "c", "x"), None), check_vma=False
    )
```

```python
import functools
import math

import jax
import jax.numpy as jnp
from jax import lax
from jax.experimental import pallas as pl
from jax.experimental.pallas import tpu as pltpu
from jax.sharding import Mesh, PartitionSpec as P

NZ, NY, NC = 8, 4, 2
DB, DN, ROPE, R = 128, 64, 64, 512
norm_eps = 1e-06
rope_base = 500000.0
low = -1e30
LOG2E = math.log2(math.e)
SP = ("z", "y", "c")


def rms_scale(values, norm_gain):
    return (
        values * lax.rsqrt(jnp.mean(values * values, axis=-1, keepdims=True) + norm_eps) * norm_gain
    )


def shift(value, axis, by):
    size = lax.axis_size(axis)
    return lax.ppermute(value, axis, [(i, (i + by) % size) for i in range(size)])


def across(value):
    return lax.ppermute(value, "c", [(0, 1), (1, 0)])


def attention(where, own, queries, wk, wvt, cosine, sine):
    rows = own.shape[0]
    half = rows // 2
    stage = lax.optimization_barrier
    up1, down1, q1, q3, o0 = stage(
        (
            shift(own, "z", 1),
            shift(own, "z", -1),
            shift(queries, "y", 1),
            shift(queries, "y", -1),
            across(own),
        )
    )
    up2, down2, q2a, q2b, o1, o7 = stage(
        (
            shift(up1, "z", 1),
            shift(down1, "z", -1),
            shift(q1[:half], "y", 1),
            shift(q3[half:], "y", -1),
            across(up1),
            across(down1),
        )
    )
    qt, *state = attend(
        where,
        (queries, q1, q2a, q2b, q3, cosine, sine),
        ((own,), (o0,), (up1,), (o1,)),
        wk,
        wvt,
        rows,
        first=True,
    )
    up3, down3, o2, o6, *state = stage(
        (shift(up2, "z", 1), shift(down2, "z", -1), across(up2), across(down2), *state)
    )
    state = attend(
        where, (qt, *state), ((up2,), (o2,), (down1,), (o7,)), wk, wvt, rows, reach=(2, 7)
    )
    far_a, far_b, o3, o5, *state = stage(
        (
            shift(up3[:half], "z", 1),
            shift(down3[half:], "z", -1),
            across(up3),
            across(down3),
            *state,
        )
    )
    last = ((up3,), (o3,), (down2,), (o6,))
    last += ((far_a, far_b), (across(far_a), across(far_b)), (down3,), (o5,))
    return attend(
        where, (qt, *state), last, wk, wvt, rows, last=True, reach=(3, 6), limit=48
    )[0]


def attend_kernel(where_ref, *refs, rows, first, last, reach):
    f32, bf16 = jnp.float32, jnp.bfloat16
    z, y, c = where_ref[0], where_ref[1], where_ref[2]
    nq, half = NY * rows, 2 * rows
    nk = 2 * half
    tile = 256
    refs = list(refs)

    def take(count):
        out = refs[:count]
        del refs[:count]
        return out

    if first:
        q_refs = take(5)
        cos_ref, sin_ref = take(2)
    else:
        qt_ref, acc_in, m_in, l_in = take(4)
    pieces = [take(len(p)) for p in part_pieces(first, last)]
    wk_ref, wvt_ref = take(2)
    if first:
        qt_ref, acc_ref, m_ref, l_ref = take(4)
        (queries_ref,) = take(1)
    elif last:
        (out_ref,) = take(1)
        acc_ref, m_ref, l_ref = take(3)
    else:
        acc_ref, m_ref, l_ref = take(3)
    lat_ref, kc_ref, vt_ref, sems = take(4)

    copies = []

    def bring(r, to):
        copies.append(pltpu.make_async_copy(r, to, sems.at[len(copies)]))
        copies[-1].start()

    if first:
        at = 0
        for r in q_refs:
            bring(r, queries_ref.at[at : at + r.shape[0]])
            at += r.shape[0]
    at = 0
    for block in pieces:
        for r in block:
            bring(r, lat_ref.at[at : at + r.shape[0]])
            at += r.shape[0]

    if first:
        for copy in copies[:5]:
            copy.wait()
        qt = queries_ref[...].astype(f32).T
        cosine, sine = cos_ref[...], sin_ref[...]

        def rotated(at):
            a, b = qt[at : at + 32], qt[at + 32 : at + 64]
            return (a * cosine - b * sine).astype(bf16), (b * cosine + a * sine).astype(bf16)

        zeros = jnp.zeros((64, nq), bf16)
        for h in range(4):
            if h < 2:
                at = h * (DB + ROPE)
                qt_ref[h, 0:128] = qt[at : at + DB].astype(bf16)
                one, two = rotated(at + DB)
            else:
                at = 2 * (DB + ROPE) + (h - 2) * (DN + ROPE)
                used, others = (h - 2) * 64, (3 - h) * 64
                qt_ref[h, used : used + 64] = qt[at : at + DN].astype(bf16)
                qt_ref[h, others : others + 64] = zeros
                one, two = rotated(at + DN)
            qt_ref[h, 128:160] = one
            qt_ref[h, 160:192] = two
            qt_ref[h, 192:256] = zeros
        acc_ref[...] = jnp.zeros_like(acc_ref)
        l_ref[...] = jnp.zeros_like(l_ref)
        m_ref[...] = jnp.full_like(m_ref, low)
        for copy in copies[5:]:
            copy.wait()
    else:
        acc_ref[...] = acc_in[...]
        m_ref[...] = m_in[...]
        l_ref[...] = l_in[...]
        for copy in copies:
            copy.wait()

    def step(at, seen):
        chunk = lat_ref[pl.ds(at, nk), :]
        normed, rope = chunk[:, :R], chunk[:, R:]
        keys = jnp.dot(normed, wk_ref[...], preferred_element_type=f32).astype(bf16)
        for k in range(3):
            kc_ref[k, :, 0:128] = keys[:, 128 * k : 128 * (k + 1)]
            kc_ref[k, :, 128:256] = rope
        vt_ref[...] = lax.dot_general(
            wvt_ref[...], normed, (((1,), (1,)), ((), ())), preferred_element_type=f32
        ).astype(bf16)
        hide = jnp.where(seen, 0.0, low)
        keep = jnp.where(seen, 1.0, 0.0)
        if first:
            row = lax.broadcasted_iota(jnp.int32, (half, 1), 0)
            side = (row >= rows).astype(jnp.int32)
            core = c + side * (1 - 2 * c)
            key_pos = ((z * NY + y) * NC + core) * rows + row - side * rows

        def q_tile(t, carry):
            lanes = pl.ds(pl.multiple_of(t * tile, tile), tile)
            if first:
                col = lax.broadcasted_iota(jnp.int32, (1, tile), 1) + t * tile
                block = (col >= rows).astype(jnp.int32)
                block += (col >= 2 * rows).astype(jnp.int32)
                block += (col >= 3 * rows).astype(jnp.int32)
                yq = y - block
                yq = jnp.where(yq < 0, yq + NY, yq)
                q_pos = ((z * NY + yq) * NC + c) * rows + col - block * rows
                allowed = key_pos <= q_pos

            def scores(h):
                return jnp.dot(
                    kc_ref[min(h, 2)], qt_ref[h, :, lanes], preferred_element_type=f32
                )

            ahead = scores(0)
            for h in range(4):
                scale = LOG2E * ((DB if h < 2 else DN) + ROPE) ** (-0.5)
                s0, s1 = ahead[:half], ahead[half:]
                if h < 3:
                    ahead = scores(h + 1)
                if first:
                    s0 = jnp.where(allowed, s0, low)
                s1 = s1 + hide
                old = m_ref[h : h + 1, lanes]
                new = jnp.maximum(
                    jnp.maximum(old, jnp.max(s0, axis=0, keepdims=True)),
                    jnp.max(s1, axis=0, keepdims=True),
                )
                w0 = jnp.exp2((s0 - new) * scale)
                w1 = jnp.exp2((s1 - new) * scale)
                if first:
                    w0 = jnp.where(allowed, w0, 0.0)
                    w1 = w1 * keep
                factor = jnp.exp2((old - new) * scale)
                m_ref[h : h + 1, lanes] = new
                l_ref[h : h + 1, lanes] = (
                    l_ref[h : h + 1, lanes] * factor
                    + jnp.sum(w0, axis=0, keepdims=True)
                    + jnp.sum(w1, axis=0, keepdims=True)
                )
                dims = slice(h * 128, h * 128 + 128) if h < 2 else slice(128 + h * 64, 192 + h * 64)
                weight = jnp.concatenate([w0.astype(bf16), w1.astype(bf16)], axis=0)
                acc_ref[dims, lanes] = acc_ref[dims, lanes] * factor + jnp.dot(
                    vt_ref[dims, :], weight, preferred_element_type=f32
                )
            return carry

        lax.fori_loop(0, nq // tile, q_tile, 0)

    if first:
        step(0, z >= 1)
    else:

        def one_pair(i, carry):
            dmin, dmax = reach[0] + i, reach[1] - i

            @pl.when(dmin <= z)
            def _():
                step(pl.multiple_of(i * nk, nk), dmax <= z)

            return carry

        lax.fori_loop(0, len(pieces) // 4, one_pair, 0)

    if last:
        total = l_ref[...]
        some = total > 0.0
        safe = jnp.where(some, total, 1.0)
        inverse = jnp.where(some, 1.0 / safe, 0.0)
        head = lax.broadcasted_iota(jnp.int32, (8, 1), 0)
        scale = jnp.where(head < 2, LOG2E * (DB + ROPE) ** (-0.5), LOG2E * (DN + ROPE) ** (-0.5))
        lse = jnp.where(some, m_ref[...] * scale + jnp.log2(safe), low)
        high = lse.astype(bf16).astype(f32)
        middle = (lse - high).astype(bf16).astype(f32)
        parts = [
            acc_ref[0:128] * inverse[0:1],
            acc_ref[128:256] * inverse[1:2],
            acc_ref[256:320] * inverse[2:3],
            acc_ref[320:384] * inverse[3:4],
        ]
        packed = jnp.concatenate(parts, axis=0).T.astype(bf16)
        tail = lse - high - middle
        for e in range(NY):
            yq = y - e
            yq = jnp.where(yq < 0, yq + NY, yq)
            span = slice(e * rows, (e + 1) * rows)
            above = jnp.concatenate([high[0:4, span], middle[0:4, span]], axis=1)
            below = jnp.concatenate([tail[0:4, span], jnp.zeros((4, rows), f32)], axis=1)
            out_ref[yq, 0:rows] = packed[span]
            out_ref[yq, rows : rows + 8] = jnp.concatenate([above, below], axis=0).astype(bf16)


def part_pieces(first, last):
    if last:
        return [(0,), (0,), (0,), (0,), (0, 1), (0, 1), (0,), (0,)]
    return [(0,)] * 4


def attend(where, start, blocks, wk, wvt, rows, first=False, last=False, reach=(0, 1), limit=30):
    nq, nk = NY * rows, 4 * rows
    f32, bf16 = jnp.float32, jnp.bfloat16
    vmem = pl.BlockSpec(memory_space=pltpu.VMEM)
    hbm = pl.BlockSpec(memory_space=pltpu.HBM)
    pieces = [p for block in blocks for p in block]
    state = [((384, nq), f32), ((8, nq), f32), ((8, nq), f32)]
    queries = ((4, 256, nq), bf16)
    scratch = []
    if first:
        out = [queries] + state
        scratch.append(pltpu.VMEM((nq, 640), bf16))
        specs = [hbm] * 5 + [vmem] * 2
    elif last:
        out = [((NY, rows + 8, 2 * rows), bf16)]
        scratch += [pltpu.VMEM(*s) for s in state]
        specs = [vmem] * 4
    else:
        out = state
        specs = [vmem] * 4
    pairs = len(blocks) // 4
    scratch += [
        pltpu.VMEM((pairs * nk, 640), bf16),
        pltpu.VMEM((3, nk, 256), bf16),
        pltpu.VMEM((384, nk), bf16),
        pltpu.SemaphoreType.DMA((len(pieces) + 5 * first,)),
    ]
    result = pl.pallas_call(
        functools.partial(attend_kernel, rows=rows, first=first, last=last, reach=reach),
        out_shape=tuple(jax.ShapeDtypeStruct(*s) for s in out),
        in_specs=[pl.BlockSpec(memory_space=pltpu.SMEM)]
        + specs
        + [hbm] * len(pieces)
        + [vmem] * 2,
        out_specs=tuple(vmem for _ in out),
        scratch_shapes=scratch,
        compiler_params=pltpu.CompilerParams(
            vmem_limit_bytes=limit * 1024 * 1024
        ),
        cost_estimate=pl.CostEstimate(
            flops=pairs * 6_000_000_000, bytes_accessed=pairs * 2_000_000, transcendentals=3_000_000
        ),
        name="attend_last" if last else "attend_first" if first else "attend_next",
    )(where, *start, *pieces, wk, wvt)
    return result


def combine_kernel(part_ref, out_ref):
    f32 = jnp.float32
    rows = out_ref.shape[0]
    stats = []
    for s in range(NY):
        st = part_ref[s, rows : rows + 8, :].astype(f32)
        stats.append(st[0:4, :rows] + st[0:4, rows:] + st[4:8, :rows])
    top = functools.reduce(jnp.maximum, stats)
    weights = [jnp.exp2(st - top) for st in stats]
    inverse = 1.0 / functools.reduce(jnp.add, weights)
    table = jnp.concatenate([w * inverse for w in weights] * 2, axis=0).T
    lane = lax.broadcasted_iota(jnp.int32, (1, 128), 1)
    for k in range(3):
        total = None
        for s in range(NY):
            at = 4 * s
            if k < 2:
                factor = table[:, at + k : at + k + 1]
            else:
                factor = jnp.where(lane < 64, table[:, at + 2 : at + 3], table[:, at + 3 : at + 4])
            term = part_ref[s, 0:rows, 128 * k : 128 * (k + 1)].astype(f32) * factor
            total = term if total is None else total + term
        out_ref[:, 128 * k : 128 * (k + 1)] = total.astype(jnp.bfloat16)


def combine(parts):
    vmem = pl.BlockSpec(memory_space=pltpu.VMEM)
    return pl.pallas_call(
        combine_kernel,
        out_shape=jax.ShapeDtypeStruct((parts.shape[1] - 8, 384), jnp.bfloat16),
        in_specs=[vmem],
        out_specs=vmem,
        compiler_params=pltpu.CompilerParams(vmem_limit_bytes=8 * 1024 * 1024),
        cost_estimate=pl.CostEstimate(flops=1_000_000, bytes_accessed=1_000_000, transcendentals=0),
        name="combine",
    )(parts)


def project_own_kernel(where_ref, own_ref, broad_ref, narrow_ref, sum_ref, rest_ref, mine_ref, sems):
    x = where_ref[0]
    copies = []
    for d in range(4):
        xd = x - d
        xd = jnp.where(xd < 0, xd + 4, xd)
        to = mine_ref if d == 0 else rest_ref.at[d - 1]
        for r, size, at in ((broad_ref, 256, 0), (narrow_ref, 128, 256)):
            rows = pl.ds(pl.multiple_of(xd * size, size), size)
            copies.append(
                pltpu.make_async_copy(r.at[rows], to.at[at : at + size], sems.at[len(copies)])
            )
            copies[-1].start()
    for copy in copies[:2]:
        copy.wait()
    sum_ref[...] = jnp.dot(own_ref[...], mine_ref[...], preferred_element_type=jnp.float32)
    for copy in copies[2:]:
        copy.wait()


def project_own(where, own, out_broad, out_narrow):
    vmem = pl.BlockSpec(memory_space=pltpu.VMEM)
    hbm = pl.BlockSpec(memory_space=pltpu.HBM)
    rows, width = own.shape[0], out_broad.shape[1]
    return pl.pallas_call(
        project_own_kernel,
        out_shape=(
            jax.ShapeDtypeStruct((rows, width), jnp.float32),
            jax.ShapeDtypeStruct((3, 384, width), jnp.bfloat16),
        ),
        in_specs=[pl.BlockSpec(memory_space=pltpu.SMEM), vmem, hbm, hbm],
        out_specs=(vmem, vmem),
        scratch_shapes=[pltpu.VMEM((384, width), jnp.bfloat16), pltpu.SemaphoreType.DMA((8,))],
        compiler_params=pltpu.CompilerParams(vmem_limit_bytes=20 * 1024 * 1024),
        cost_estimate=pl.CostEstimate(
            flops=2_000_000_000, bytes_accessed=8_000_000, transcendentals=0
        ),
        name="project_own",
    )(where, own, out_broad, out_narrow)


def project_kernel(
    p1_ref, p2_ref, p3_ref, sum_ref, rest_ref, resid_ref, post_ref, gain_ref, mixed_ref, normed_ref
):
    f32, bf16 = jnp.float32, jnp.bfloat16
    projected = sum_ref[...] + jnp.dot(
        jnp.concatenate([p1_ref[...], p2_ref[...], p3_ref[...]], axis=1),
        jnp.concatenate([rest_ref[0], rest_ref[1], rest_ref[2]], axis=0),
        preferred_element_type=f32,
    )
    mixed = (resid_ref[...].astype(f32) + rms_scale(projected, post_ref[...])).astype(bf16)
    mixed_ref[...] = mixed
    normed_ref[...] = rms_scale(mixed.astype(f32), gain_ref[...]).astype(bf16)


def project(pieces, own_sum, rest, resid, post_gain, ffn_gain):
    vmem = pl.BlockSpec(memory_space=pltpu.VMEM)
    rows, width = resid.shape
    shape = jax.ShapeDtypeStruct((rows, width), jnp.bfloat16)
    return pl.pallas_call(
        project_kernel,
        out_shape=(shape, shape),
        in_specs=[vmem] * 8,
        out_specs=(vmem, vmem),
        compiler_params=pltpu.CompilerParams(vmem_limit_bytes=20 * 1024 * 1024),
        cost_estimate=pl.CostEstimate(
            flops=2 * rows * 1152 * width, bytes_accessed=8_000_000, transcendentals=0
        ),
        name="project",
    )(*pieces, own_sum, rest, resid, post_gain[None], ffn_gain[None])


def ffn_kernel(normed_ref, both_ref, out_ref, up_ref, down_ref, hidden_ref, up_sem, down_sem, *, tile):
    f32, bf16 = jnp.float32, jnp.bfloat16
    width, units = up_ref.shape
    steps = units // tile

    ahead = 4

    def up_copy(i):
        at = pl.ds(pl.multiple_of(i * tile, tile), tile)
        return pltpu.make_async_copy(both_ref.at[:, at], up_ref.at[:, at], up_sem.at[i])

    def down_copy(i):
        at = pl.ds(pl.multiple_of(i * tile, tile), tile)
        return pltpu.make_async_copy(
            both_ref.at[at, pl.ds(units, units)], down_ref.at[at, :], down_sem.at[i]
        )

    for i in range(ahead):
        up_copy(i).start()

    def first(i, carry):
        at = pl.ds(pl.multiple_of(i * tile, tile), tile)
        up_copy(i).wait()

        @pl.when(i < steps - ahead)
        def _():
            up_copy(i + ahead).start()

        @pl.when(i >= steps - ahead)
        def _():
            down_copy(i - (steps - ahead)).start()

        up = jnp.dot(normed_ref[...], up_ref[:, at], preferred_element_type=f32)
        hidden_ref[:, at] = jnp.square(jnp.maximum(up, 0.0)).astype(bf16)
        return carry

    lax.fori_loop(0, steps, first, 0)

    def second(i, carry):
        at = pl.ds(pl.multiple_of(i * tile, tile), tile)
        down_copy(i).wait()

        @pl.when(i < width // tile - ahead)
        def _():
            down_copy(i + ahead).start()

        term = lax.dot_general(
            hidden_ref[...], down_ref[at, :], (((1,), (1,)), ((), ())), preferred_element_type=f32
        )
        out_ref[:, at] = term.astype(bf16)
        return carry

    lax.fori_loop(0, width // tile, second, 0)


def feed_forward(normed, both, units):
    rows, width = normed.shape
    tile = 512
    return pl.pallas_call(
        functools.partial(ffn_kernel, tile=tile),
        out_shape=jax.ShapeDtypeStruct((rows, width), jnp.bfloat16),
        in_specs=[
            pl.BlockSpec(memory_space=pltpu.VMEM),
            pl.BlockSpec(memory_space=pltpu.HBM),
        ],
        out_specs=pl.BlockSpec(memory_space=pltpu.VMEM),
        scratch_shapes=[
            pltpu.VMEM((width, units), jnp.bfloat16),
            pltpu.VMEM((width, units), jnp.bfloat16),
            pltpu.VMEM((rows, units), jnp.bfloat16),
            pltpu.SemaphoreType.DMA((units // tile,)),
            pltpu.SemaphoreType.DMA((width // tile,)),
        ],
        compiler_params=pltpu.CompilerParams(vmem_limit_bytes=48 * 1024 * 1024),
        cost_estimate=pl.CostEstimate(
            flops=4 * rows * width * units, bytes_accessed=4 * width * units, transcendentals=0
        ),
        name="feed_forward",
    )(normed, both)


def angles(positions):
    frequency = rope_base ** (-2.0 * jnp.arange(ROPE // 2, dtype=jnp.float32) / ROPE)
    return positions.astype(jnp.float32), frequency


def local(
    resid, query_broad, query_narrow, latent, key_rope, latent_gain, key_up_broad, value_up_broad,
    key_up_narrow, value_up_narrow, out_broad, out_narrow, post_gain, ffn_gain, up_weight,
    down_weight, ffn_out_gain,
):
    f32, bf16 = jnp.float32, jnp.bfloat16
    rows = resid.shape[0]
    z, y, c = (lax.axis_index(a) for a in SP)
    first = ((z * NY + y) * NC + c) * rows
    within = jnp.arange(rows, dtype=jnp.int32)

    both = lax.all_gather(
        jnp.concatenate([up_weight, down_weight], axis=1), SP, axis=0, tiled=True
    )

    normed_latent = rms_scale(latent.astype(f32), latent_gain).astype(bf16)
    pos, frequency = angles(first + within)
    angle = pos[:, None] * frequency[None, :]
    ka, kb = key_rope[:, :32].astype(f32), key_rope[:, 32:].astype(f32)
    cosine, sine = jnp.cos(angle), jnp.sin(angle)
    key_rot = jnp.concatenate([ka * cosine - kb * sine, kb * cosine + ka * sine], axis=1)
    sent = jnp.concatenate(
        [normed_latent, key_rot.astype(bf16), jnp.zeros((rows, 64), bf16)], axis=1
    )
    block_y = jnp.mod(y - jnp.arange(NY, dtype=jnp.int32), NY)
    q_pos = ((z * NY + block_y) * NC + c)[:, None] * rows + within[None, :]
    pos, frequency = angles(q_pos.reshape(-1))
    angle = frequency[:, None] * pos[None, :]
    wk = jnp.concatenate([key_up_broad, key_up_narrow], axis=1)
    wvt = jnp.concatenate([value_up_broad, value_up_narrow], axis=1).T
    where = jnp.stack([z, y, c]).astype(jnp.int32)
    queries = jnp.concatenate([query_broad, query_narrow], axis=1)
    partial = attention(where, sent, queries, wk, wvt, jnp.cos(angle), jnp.sin(angle))
    parts = lax.all_to_all(partial, "y", 0, 0, tiled=True)
    attn = combine(parts)
    pieces = [shift(attn, "x", d) for d in (1, 2, 3)]
    nx, x = lax.axis_size("x"), lax.axis_index("x")
    own_sum, rest = project_own(x[None].astype(jnp.int32), attn, out_broad, out_narrow)
    mixed, normed = project(pieces, own_sum, rest, resid, post_gain, ffn_gain)
    units = up_weight.shape[1]
    share = feed_forward(normed, both, units)
    own_rows = rows // nx
    shares = lax.all_to_all(share.reshape(nx, own_rows, -1), "x", 0, 0, tiled=True)
    ffn = jnp.sum(shares.astype(f32), axis=0)
    own = lax.dynamic_slice_in_dim(mixed, x * own_rows, own_rows, 0)
    return (own.astype(f32) + rms_scale(ffn, ffn_out_gain)).astype(bf16)


def solution(mesh):
    grid = Mesh(mesh.devices.reshape(NZ, NY, NC, -1), ("z", "y", "c", "x"))
    row, split, heads = P(SP, None), P(SP, "x"), P(None, "x")
    in_specs = (
        row, split, split, row, row, P(), heads, heads, heads, heads, P(), P(), P(), P(),
        split, split, P(),
    )
    return jax.shard_map(
        local, mesh=grid, in_specs=in_specs, out_specs=P(("z", "y", "c", "x"), None), check_vma=False
    )
```

```python
import functools
import math

import jax
import jax.numpy as jnp
from jax import lax
from jax.experimental import pallas as pl
from jax.experimental.pallas import tpu as pltpu
from jax.sharding import Mesh, PartitionSpec as P

NZ, NY, NC = 8, 4, 2
DB, DN, ROPE, R = 128, 64, 64, 512
norm_eps = 1e-06
rope_base = 500000.0
low = -1e30
LOG2E = math.log2(math.e)
SP = ("z", "y", "c")


def rms_scale(values, norm_gain):
    return (
        values * lax.rsqrt(jnp.mean(values * values, axis=-1, keepdims=True) + norm_eps) * norm_gain
    )


def shift(value, axis, by, to=None):
    size = lax.axis_size(axis)
    pairs = [(i, (i + by) % size) for i in range(size)]
    return lax.ppermute(value, axis, [p for p in pairs if to is None or p[1] in to])


def across(value):
    return lax.ppermute(value, "c", [(0, 1), (1, 0)])


def attention(where, own, queries, wk, wvt, cosine, sine):
    rows = own.shape[0]
    half = rows // 2
    stage = lax.optimization_barrier
    up1, down1, q1, q3, o0 = stage(
        (
            shift(own, "z", 1, (1, 2, 3, 4, 5, 6, 7)),
            shift(own, "z", -1, (7, 0, 1, 2)),
            shift(queries, "y", 1),
            shift(queries, "y", -1),
            across(own),
        )
    )
    up2, down2, q2a, q2b, o1, o7 = stage(
        (
            shift(up1, "z", 1, (2, 3, 4, 5, 6, 7)),
            shift(down1, "z", -1, (6, 7, 0, 1)),
            shift(q1[:half], "y", 1),
            shift(q3[half:], "y", -1),
            across(up1),
            across(down1),
        )
    )
    qt, *state = attend(
        where,
        (queries, q1, q2a, q2b, q3, cosine, sine),
        (own, o0, up1, o1),
        wk,
        wvt,
        rows,
        first=True,
    )
    up3, down3, o2, o6, *state = stage(
        (
            shift(up2, "z", 1, (3, 4, 5, 6, 7)),
            shift(down2, "z", -1, (5, 6, 7, 0)),
            across(up2),
            across(down2),
            *state,
        )
    )
    state = attend(
        where, (qt, *state), (up2, o2, down1, o7), wk, wvt, rows, reach=(2, 7)
    )
    down4, o3, o5, *state = stage(
        (
            shift(down3, "z", -1, (4, 5, 6, 7)),
            across(up3),
            across(down3),
            *state,
        )
    )
    last = (up3, o3, down2, o6, down4, across(down4), down3, o5)
    return attend(
        where, (qt, *state), last, wk, wvt, rows, last=True, reach=(3, 6), limit=48
    )[0]


def attend_kernel(where_ref, *refs, rows, first, last, reach):
    f32, bf16 = jnp.float32, jnp.bfloat16
    z, y, c = where_ref[0], where_ref[1], where_ref[2]
    nq, half = NY * rows, 2 * rows
    nk = 2 * half
    tile = 256
    refs = list(refs)

    def take(count):
        out = refs[:count]
        del refs[:count]
        return out

    if first:
        q_refs = take(5)
        cos_ref, sin_ref = take(2)
    else:
        qt_ref, acc_in, m_in, l_in = take(4)
    pieces = take(8 if last else 4)
    wk_ref, wvt_ref = take(2)
    if first:
        qt_ref, acc_ref, m_ref, l_ref = take(4)
        (queries_ref,) = take(1)
    elif last:
        (out_ref,) = take(1)
        acc_ref, m_ref, l_ref = take(3)
    else:
        acc_ref, m_ref, l_ref = take(3)
    lat_ref, kc_ref, vt_ref, sems = take(4)

    copies = []

    def bring(r, to):
        copies.append(pltpu.make_async_copy(r, to, sems.at[len(copies)]))
        copies[-1].start()

    if first:
        at = 0
        for r in q_refs:
            bring(r, queries_ref.at[at : at + r.shape[0]])
            at += r.shape[0]
    at = 0
    for r in pieces:
        bring(r, lat_ref.at[at : at + rows])
        at += rows

    if first:
        for copy in copies[:5]:
            copy.wait()
        qt = queries_ref[...].astype(f32).T
        cosine, sine = cos_ref[...], sin_ref[...]

        def rotated(at):
            a, b = qt[at : at + 32], qt[at + 32 : at + 64]
            return (a * cosine - b * sine).astype(bf16), (b * cosine + a * sine).astype(bf16)

        zeros = jnp.zeros((64, nq), bf16)
        for h in range(4):
            if h < 2:
                at = h * (DB + ROPE)
                qt_ref[h, 0:128] = qt[at : at + DB].astype(bf16)
                one, two = rotated(at + DB)
            else:
                at = 2 * (DB + ROPE) + (h - 2) * (DN + ROPE)
                used, others = (h - 2) * 64, (3 - h) * 64
                qt_ref[h, used : used + 64] = qt[at : at + DN].astype(bf16)
                qt_ref[h, others : others + 64] = zeros
                one, two = rotated(at + DN)
            qt_ref[h, 128:160] = one
            qt_ref[h, 160:192] = two
            qt_ref[h, 192:256] = zeros
        acc_ref[...] = jnp.zeros_like(acc_ref)
        l_ref[...] = jnp.zeros_like(l_ref)
        m_ref[...] = jnp.full_like(m_ref, low)
        for copy in copies[5:]:
            copy.wait()
    else:
        acc_ref[...] = acc_in[...]
        m_ref[...] = m_in[...]
        l_ref[...] = l_in[...]
        for copy in copies:
            copy.wait()

    def step(at, seen):
        chunk = lat_ref[pl.ds(at, nk), :]
        normed, rope = chunk[:, :R], chunk[:, R:]
        keys = jnp.dot(normed, wk_ref[...], preferred_element_type=f32).astype(bf16)
        for k in range(3):
            kc_ref[k, :, 0:128] = keys[:, 128 * k : 128 * (k + 1)]
            kc_ref[k, :, 128:256] = rope
        vt_ref[...] = lax.dot_general(
            wvt_ref[...], normed, (((1,), (1,)), ((), ())), preferred_element_type=f32
        ).astype(bf16)
        hide = jnp.where(seen, 0.0, low)
        keep = jnp.where(seen, 1.0, 0.0)
        if first:
            row = lax.broadcasted_iota(jnp.int32, (half, 1), 0)
            side = (row >= rows).astype(jnp.int32)
            core = c + side * (1 - 2 * c)
            key_pos = ((z * NY + y) * NC + core) * rows + row - side * rows

        def q_tile(t, carry):
            lanes = pl.ds(pl.multiple_of(t * tile, tile), tile)
            if first:
                col = lax.broadcasted_iota(jnp.int32, (1, tile), 1) + t * tile
                block = (col >= rows).astype(jnp.int32)
                block += (col >= 2 * rows).astype(jnp.int32)
                block += (col >= 3 * rows).astype(jnp.int32)
                yq = y - block
                yq = jnp.where(yq < 0, yq + NY, yq)
                q_pos = ((z * NY + yq) * NC + c) * rows + col - block * rows
                allowed = key_pos <= q_pos

            def scores(h):
                return jnp.dot(
                    kc_ref[min(h, 2)], qt_ref[h, :, lanes], preferred_element_type=f32
                )

            ahead = scores(0)
            for h in range(4):
                scale = LOG2E * ((DB if h < 2 else DN) + ROPE) ** (-0.5)
                s0, s1 = ahead[:half], ahead[half:]
                if h < 3:
                    ahead = scores(h + 1)
                if first:
                    s0 = jnp.where(allowed, s0, low)
                s1 = s1 + hide
                old = m_ref[h : h + 1, lanes]
                new = jnp.maximum(
                    jnp.maximum(old, jnp.max(s0, axis=0, keepdims=True)),
                    jnp.max(s1, axis=0, keepdims=True),
                )
                w0 = jnp.exp2((s0 - new) * scale)
                w1 = jnp.exp2((s1 - new) * scale)
                if first:
                    w0 = jnp.where(allowed, w0, 0.0)
                    w1 = w1 * keep
                factor = jnp.exp2((old - new) * scale)
                m_ref[h : h + 1, lanes] = new
                l_ref[h : h + 1, lanes] = (
                    l_ref[h : h + 1, lanes] * factor
                    + jnp.sum(w0, axis=0, keepdims=True)
                    + jnp.sum(w1, axis=0, keepdims=True)
                )
                dims = slice(h * 128, h * 128 + 128) if h < 2 else slice(128 + h * 64, 192 + h * 64)
                weight = jnp.concatenate([w0.astype(bf16), w1.astype(bf16)], axis=0)
                acc_ref[dims, lanes] = acc_ref[dims, lanes] * factor + jnp.dot(
                    vt_ref[dims, :], weight, preferred_element_type=f32
                )
            return carry

        lax.fori_loop(0, nq // tile, q_tile, 0)

    if first:
        step(0, z >= 1)
    else:

        def one_pair(i, carry):
            dmin, dmax = reach[0] + i, reach[1] - i

            @pl.when(dmin <= z)
            def _():
                step(pl.multiple_of(i * nk, nk), dmax <= z)

            return carry

        lax.fori_loop(0, len(pieces) // 4, one_pair, 0)

    if last:
        total = l_ref[...]
        some = total > 0.0
        safe = jnp.where(some, total, 1.0)
        inverse = jnp.where(some, 1.0 / safe, 0.0)
        head = lax.broadcasted_iota(jnp.int32, (8, 1), 0)
        scale = jnp.where(head < 2, LOG2E * (DB + ROPE) ** (-0.5), LOG2E * (DN + ROPE) ** (-0.5))
        lse = jnp.where(some, m_ref[...] * scale + jnp.log2(safe), low)
        high = lse.astype(bf16).astype(f32)
        middle = (lse - high).astype(bf16).astype(f32)
        parts = [
            acc_ref[0:128] * inverse[0:1],
            acc_ref[128:256] * inverse[1:2],
            acc_ref[256:320] * inverse[2:3],
            acc_ref[320:384] * inverse[3:4],
        ]
        packed = jnp.concatenate(parts, axis=0).T.astype(bf16)
        tail = lse - high - middle
        for e in range(NY):
            yq = y - e
            yq = jnp.where(yq < 0, yq + NY, yq)
            span = slice(e * rows, (e + 1) * rows)
            above = jnp.concatenate([high[0:4, span], middle[0:4, span]], axis=1)
            below = jnp.concatenate([tail[0:4, span], jnp.zeros((4, rows), f32)], axis=1)
            out_ref[yq, 0:rows] = packed[span]
            out_ref[yq, rows : rows + 8] = jnp.concatenate([above, below], axis=0).astype(bf16)


def attend(where, start, blocks, wk, wvt, rows, first=False, last=False, reach=(0, 1), limit=30):
    nq, nk = NY * rows, 4 * rows
    f32, bf16 = jnp.float32, jnp.bfloat16
    vmem = pl.BlockSpec(memory_space=pltpu.VMEM)
    hbm = pl.BlockSpec(memory_space=pltpu.HBM)
    pieces = blocks
    state = [((384, nq), f32), ((8, nq), f32), ((8, nq), f32)]
    queries = ((4, 256, nq), bf16)
    scratch = []
    if first:
        out = [queries] + state
        scratch.append(pltpu.VMEM((nq, 640), bf16))
        specs = [hbm] * 5 + [vmem] * 2
    elif last:
        out = [((NY, rows + 8, 2 * rows), bf16)]
        scratch += [pltpu.VMEM(*s) for s in state]
        specs = [vmem] * 4
    else:
        out = state
        specs = [vmem] * 4
    pairs = len(blocks) // 4
    scratch += [
        pltpu.VMEM((pairs * nk, 640), bf16),
        pltpu.VMEM((3, nk, 256), bf16),
        pltpu.VMEM((384, nk), bf16),
        pltpu.SemaphoreType.DMA((len(pieces) + 5 * first,)),
    ]
    result = pl.pallas_call(
        functools.partial(attend_kernel, rows=rows, first=first, last=last, reach=reach),
        out_shape=tuple(jax.ShapeDtypeStruct(*s) for s in out),
        in_specs=[pl.BlockSpec(memory_space=pltpu.SMEM)]
        + specs
        + [hbm] * len(pieces)
        + [vmem] * 2,
        out_specs=tuple(vmem for _ in out),
        scratch_shapes=scratch,
        compiler_params=pltpu.CompilerParams(
            vmem_limit_bytes=limit * 1024 * 1024
        ),
        cost_estimate=pl.CostEstimate(
            flops=pairs * 6_000_000_000, bytes_accessed=pairs * 2_000_000, transcendentals=3_000_000
        ),
        name="attend_last" if last else "attend_first" if first else "attend_next",
    )(where, *start, *pieces, wk, wvt)
    return result


def combine_kernel(part_ref, out_ref):
    f32 = jnp.float32
    rows = out_ref.shape[0]
    stats = []
    for s in range(NY):
        st = part_ref[s, rows : rows + 8, :].astype(f32)
        stats.append(st[0:4, :rows] + st[0:4, rows:] + st[4:8, :rows])
    top = functools.reduce(jnp.maximum, stats)
    weights = [jnp.exp2(st - top) for st in stats]
    inverse = 1.0 / functools.reduce(jnp.add, weights)
    table = jnp.concatenate([w * inverse for w in weights] * 2, axis=0).T
    lane = lax.broadcasted_iota(jnp.int32, (1, 128), 1)
    for k in range(3):
        total = None
        for s in range(NY):
            at = 4 * s
            if k < 2:
                factor = table[:, at + k : at + k + 1]
            else:
                factor = jnp.where(lane < 64, table[:, at + 2 : at + 3], table[:, at + 3 : at + 4])
            term = part_ref[s, 0:rows, 128 * k : 128 * (k + 1)].astype(f32) * factor
            total = term if total is None else total + term
        out_ref[:, 128 * k : 128 * (k + 1)] = total.astype(jnp.bfloat16)


def combine(parts):
    vmem = pl.BlockSpec(memory_space=pltpu.VMEM)
    return pl.pallas_call(
        combine_kernel,
        out_shape=jax.ShapeDtypeStruct((parts.shape[1] - 8, 384), jnp.bfloat16),
        in_specs=[vmem],
        out_specs=vmem,
        compiler_params=pltpu.CompilerParams(vmem_limit_bytes=8 * 1024 * 1024),
        cost_estimate=pl.CostEstimate(flops=1_000_000, bytes_accessed=1_000_000, transcendentals=0),
        name="combine",
    )(parts)


def project_own_kernel(where_ref, own_ref, broad_ref, narrow_ref, sum_ref, rest_ref, mine_ref, sems):
    x = where_ref[0]
    copies = []
    for d in range(4):
        xd = x - d
        xd = jnp.where(xd < 0, xd + 4, xd)
        to = mine_ref if d == 0 else rest_ref.at[d - 1]
        for r, size, at in ((broad_ref, 256, 0), (narrow_ref, 128, 256)):
            rows = pl.ds(pl.multiple_of(xd * size, size), size)
            copies.append(
                pltpu.make_async_copy(r.at[rows], to.at[at : at + size], sems.at[len(copies)])
            )
            copies[-1].start()
    for copy in copies[:2]:
        copy.wait()
    sum_ref[...] = jnp.dot(own_ref[...], mine_ref[...], preferred_element_type=jnp.float32)
    for copy in copies[2:]:
        copy.wait()


def project_own(where, own, out_broad, out_narrow):
    vmem = pl.BlockSpec(memory_space=pltpu.VMEM)
    hbm = pl.BlockSpec(memory_space=pltpu.HBM)
    rows, width = own.shape[0], out_broad.shape[1]
    return pl.pallas_call(
        project_own_kernel,
        out_shape=(
            jax.ShapeDtypeStruct((rows, width), jnp.float32),
            jax.ShapeDtypeStruct((3, 384, width), jnp.bfloat16),
        ),
        in_specs=[pl.BlockSpec(memory_space=pltpu.SMEM), vmem, hbm, hbm],
        out_specs=(vmem, vmem),
        scratch_shapes=[pltpu.VMEM((384, width), jnp.bfloat16), pltpu.SemaphoreType.DMA((8,))],
        compiler_params=pltpu.CompilerParams(vmem_limit_bytes=20 * 1024 * 1024),
        cost_estimate=pl.CostEstimate(
            flops=2_000_000_000, bytes_accessed=8_000_000, transcendentals=0
        ),
        name="project_own",
    )(where, own, out_broad, out_narrow)


def project_kernel(
    p1_ref, p2_ref, p3_ref, sum_ref, rest_ref, resid_ref, post_ref, gain_ref, mixed_ref, normed_ref
):
    f32, bf16 = jnp.float32, jnp.bfloat16
    projected = sum_ref[...] + jnp.dot(
        jnp.concatenate([p1_ref[...], p2_ref[...], p3_ref[...]], axis=1),
        jnp.concatenate([rest_ref[0], rest_ref[1], rest_ref[2]], axis=0),
        preferred_element_type=f32,
    )
    mixed = (resid_ref[...].astype(f32) + rms_scale(projected, post_ref[...])).astype(bf16)
    mixed_ref[...] = mixed
    normed_ref[...] = rms_scale(mixed.astype(f32), gain_ref[...]).astype(bf16)


def project(pieces, own_sum, rest, resid, post_gain, ffn_gain):
    vmem = pl.BlockSpec(memory_space=pltpu.VMEM)
    rows, width = resid.shape
    shape = jax.ShapeDtypeStruct((rows, width), jnp.bfloat16)
    return pl.pallas_call(
        project_kernel,
        out_shape=(shape, shape),
        in_specs=[vmem] * 8,
        out_specs=(vmem, vmem),
        compiler_params=pltpu.CompilerParams(vmem_limit_bytes=20 * 1024 * 1024),
        cost_estimate=pl.CostEstimate(
            flops=2 * rows * 1152 * width, bytes_accessed=8_000_000, transcendentals=0
        ),
        name="project",
    )(*pieces, own_sum, rest, resid, post_gain[None], ffn_gain[None])


def ffn_kernel(where_ref, *refs, tile, first):
    f32, bf16 = jnp.float32, jnp.bfloat16
    if first:
        normed_ref, both_ref, *out_refs = refs[:6]
        hidden_ref, up_ref, down_ref, sum_ref, up_sem, down_sem = refs[6:]
    else:
        hidden_ref, both_ref, *out_refs = refs[:6]
        down_ref, sum_ref, down_sem = refs[6:]
    units = hidden_ref.shape[1]
    width = both_ref.shape[0]
    steps, parts = units // tile, width // tile // 2
    skipped = 0 if first else parts

    def down_copy(i):
        at = pl.ds(pl.multiple_of((i + skipped) * tile, tile), tile)
        to = pl.ds(pl.multiple_of(i * tile, tile), tile)
        return pltpu.make_async_copy(
            both_ref.at[at, pl.ds(units, units)], down_ref.at[to, :], down_sem.at[i]
        )

    if first:

        def up_copy(i):
            at = pl.ds(pl.multiple_of(i * tile, tile), tile)
            return pltpu.make_async_copy(both_ref.at[:, at], up_ref.at[:, at], up_sem.at[i])

        for i in range(steps):
            up_copy(i).start()

        def hide(i, carry):
            at = pl.ds(pl.multiple_of(i * tile, tile), tile)
            up_copy(i).wait()

            @pl.when(i < parts)
            def _():
                down_copy(i).start()

            up = jnp.dot(normed_ref[...], up_ref[:, at], preferred_element_type=f32)
            hidden_ref[:, at] = jnp.square(jnp.maximum(up, 0.0)).astype(bf16)
            return carry

        lax.fori_loop(0, steps, hide, 0)
    else:
        for i in range(parts):
            down_copy(i).start()

    def multiply(i, carry):
        at = pl.ds(pl.multiple_of(i * tile, tile), tile)
        down_copy(i).wait()
        term = lax.dot_general(
            hidden_ref[...], down_ref[at, :], (((1,), (1,)), ((), ())), preferred_element_type=f32
        )
        sum_ref[:, at] = term.astype(bf16)
        return carry

    lax.fori_loop(0, parts, multiply, 0)

    x = where_ref[0]
    rows = out_refs[0].shape[0]
    for d, out_ref in enumerate(out_refs):
        xd = x + d
        xd = jnp.where(xd >= 4, xd - 4, xd)
        out_ref[...] = sum_ref[pl.ds(pl.multiple_of(xd * rows, rows), rows), :]


def feed_forward(where, operand, both, units, first):
    rows, width = operand.shape[0], both.shape[0]
    tile, bf16 = 512, jnp.bfloat16
    vmem = pl.BlockSpec(memory_space=pltpu.VMEM)
    half = width // 2
    out = [jax.ShapeDtypeStruct((rows // 4, half), bf16)] * 4
    scratch = [
        pltpu.VMEM((half, units), bf16),
        pltpu.VMEM((rows, half), bf16),
        pltpu.SemaphoreType.DMA((half // tile,)),
    ]
    if first:
        out.append(jax.ShapeDtypeStruct((rows, units), bf16))
        up_sem = pltpu.SemaphoreType.DMA((units // tile,))
        scratch = [pltpu.VMEM((width, units), bf16), *scratch[:2], up_sem, scratch[2]]
    return pl.pallas_call(
        functools.partial(ffn_kernel, tile=tile, first=first),
        out_shape=tuple(out),
        in_specs=[
            pl.BlockSpec(memory_space=pltpu.SMEM),
            vmem,
            pl.BlockSpec(memory_space=pltpu.HBM),
        ],
        out_specs=tuple(vmem for _ in out),
        scratch_shapes=scratch,
        compiler_params=pltpu.CompilerParams(vmem_limit_bytes=50 * 1024 * 1024),
        cost_estimate=pl.CostEstimate(
            flops=2_000_000_000, bytes_accessed=4 * width * units, transcendentals=0
        ),
        name="feed_forward_first" if first else "feed_forward_second",
    )(where, operand, both)


def angles(positions):
    frequency = rope_base ** (-2.0 * jnp.arange(ROPE // 2, dtype=jnp.float32) / ROPE)
    return positions.astype(jnp.float32), frequency


def local(
    resid, query_broad, query_narrow, latent, key_rope, latent_gain, key_up_broad, value_up_broad,
    key_up_narrow, value_up_narrow, out_broad, out_narrow, post_gain, ffn_gain, up_weight,
    down_weight, ffn_out_gain,
):
    f32, bf16 = jnp.float32, jnp.bfloat16
    rows = resid.shape[0]
    z, y, c = (lax.axis_index(a) for a in SP)
    first = ((z * NY + y) * NC + c) * rows
    within = jnp.arange(rows, dtype=jnp.int32)

    both = lax.all_gather(
        jnp.concatenate([up_weight, down_weight], axis=1), SP, axis=0, tiled=True
    )

    normed_latent = rms_scale(latent.astype(f32), latent_gain).astype(bf16)
    pos, frequency = angles(first + within)
    angle = pos[:, None] * frequency[None, :]
    ka, kb = key_rope[:, :32].astype(f32), key_rope[:, 32:].astype(f32)
    cosine, sine = jnp.cos(angle), jnp.sin(angle)
    key_rot = jnp.concatenate([ka * cosine - kb * sine, kb * cosine + ka * sine], axis=1)
    sent = jnp.concatenate(
        [normed_latent, key_rot.astype(bf16), jnp.zeros((rows, 64), bf16)], axis=1
    )
    block_y = jnp.mod(y - jnp.arange(NY, dtype=jnp.int32), NY)
    q_pos = ((z * NY + block_y) * NC + c)[:, None] * rows + within[None, :]
    pos, frequency = angles(q_pos.reshape(-1))
    angle = frequency[:, None] * pos[None, :]
    wk = jnp.concatenate([key_up_broad, key_up_narrow], axis=1)
    wvt = jnp.concatenate([value_up_broad, value_up_narrow], axis=1).T
    where = jnp.stack([z, y, c]).astype(jnp.int32)
    queries = jnp.concatenate([query_broad, query_narrow], axis=1)
    partial = attention(where, sent, queries, wk, wvt, jnp.cos(angle), jnp.sin(angle))
    parts = lax.all_to_all(partial, "y", 0, 0, tiled=True)
    attn = combine(parts)
    pieces = [shift(attn, "x", d) for d in (1, 2, 3)]
    nx, x = lax.axis_size("x"), lax.axis_index("x")
    place = x[None].astype(jnp.int32)
    own_sum, rest = project_own(place, attn, out_broad, out_narrow)
    mixed, normed = project(pieces, own_sum, rest, resid, post_gain, ffn_gain)
    units = up_weight.shape[1]
    *first, hidden = feed_forward(place, normed, both, units, True)
    sums = []
    come = [shift(first[d], "x", d) for d in (1, 2, 3)]
    second = feed_forward(place, hidden, both, units, False)
    for own, others in ((first[0], come), (second[0], None)):
        if others is None:
            others = [shift(second[d], "x", d) for d in (1, 2, 3)]
        sums.append(sum([o.astype(f32) for o in others], own.astype(f32)))
    ffn = jnp.concatenate(sums, axis=1)
    own_rows = rows // nx
    own = lax.dynamic_slice_in_dim(mixed, x * own_rows, own_rows, 0)
    return (own.astype(f32) + rms_scale(ffn, ffn_out_gain)).astype(bf16)


def solution(mesh):
    grid = Mesh(mesh.devices.reshape(NZ, NY, NC, -1), ("z", "y", "c", "x"))
    row, split, heads = P(SP, None), P(SP, "x"), P(None, "x")
    in_specs = (
        row, split, split, row, row, P(), heads, heads, heads, heads, P(), P(), P(), P(),
        split, split, P(),
    )
    return jax.shard_map(
        local, mesh=grid, in_specs=in_specs, out_specs=P(("z", "y", "c", "x"), None), check_vma=False
    )
```

```python
import functools
import math

import jax
import jax.numpy as jnp
from jax import lax
from jax.experimental import pallas as pl
from jax.experimental.pallas import tpu as pltpu
from jax.sharding import Mesh, PartitionSpec as P

NZ, NY, NC = 8, 4, 2
DB, DN, ROPE, R = 128, 64, 64, 512
norm_eps = 1e-06
rope_base = 500000.0
low = -1e30
LOG2E = math.log2(math.e)
SP = ("z", "y", "c")


def rms_scale(values, norm_gain):
    return (
        values * lax.rsqrt(jnp.mean(values * values, axis=-1, keepdims=True) + norm_eps) * norm_gain
    )


def shift(value, axis, by, to=None):
    size = lax.axis_size(axis)
    pairs = [(i, (i + by) % size) for i in range(size)]
    return lax.ppermute(value, axis, [p for p in pairs if to is None or p[1] in to])


def across(value):
    return lax.ppermute(value, "c", [(0, 1), (1, 0)])


def attention(where, own, queries, wk, wvt, cosine, sine):
    rows = own.shape[0]
    stage = lax.optimization_barrier
    q1, q3, q2 = shift(queries, "y", 1), shift(queries, "y", -1), shift(queries, "y", 2)
    up1, down1, o0 = stage(
        (
            shift(own, "z", 1, (1, 2, 3, 4, 5, 6, 7)),
            shift(own, "z", -1, (7, 0, 1, 2)),
            across(own),
        )
    )
    up2, down2, q1, q2, q3, o1, o7 = stage(
        (
            shift(up1, "z", 1, (2, 3, 4, 5, 6, 7)),
            shift(down1, "z", -1, (6, 7, 0, 1)),
            q1,
            q2,
            q3,
            across(up1),
            across(down1),
        )
    )
    qt, *state = attend(
        where,
        (queries, q1, q2, q3, cosine, sine),
        (own, o0, up1, o1),
        wk,
        wvt,
        rows,
        first=True,
    )
    up3, down3, o2, o6, *state = stage(
        (
            shift(up2, "z", 1, (3, 4, 5, 6, 7)),
            shift(down2, "z", -1, (5, 6, 7, 0)),
            across(up2),
            across(down2),
            *state,
        )
    )
    state = attend(
        where, (qt, *state), (up2, o2, down1, o7), wk, wvt, rows, reach=(2, 7)
    )
    down4, o3, o5, *state = stage(
        (
            shift(down3, "z", -1, (4, 5, 6, 7)),
            across(up3),
            across(down3),
            *state,
        )
    )
    last = (up3, o3, down2, o6, down4, across(down4), down3, o5)
    return attend(
        where, (qt, *state), last, wk, wvt, rows, last=True, reach=(3, 6), limit=48
    )[0]


def attend_kernel(where_ref, *refs, rows, first, last, reach):
    f32, bf16 = jnp.float32, jnp.bfloat16
    z, y, c = where_ref[0], where_ref[1], where_ref[2]
    nq, half = NY * rows, 2 * rows
    nk = 2 * half
    tile = 256
    refs = list(refs)

    def take(count):
        out = refs[:count]
        del refs[:count]
        return out

    if first:
        q_refs = take(4)
        cos_ref, sin_ref = take(2)
    else:
        qt_ref, acc_in, m_in, l_in = take(4)
    pieces = take(8 if last else 4)
    wk_ref, wvt_ref = take(2)
    if first:
        qt_ref, acc_ref, m_ref, l_ref = take(4)
        (queries_ref,) = take(1)
    elif last:
        (out_ref,) = take(1)
        acc_ref, m_ref, l_ref = take(3)
    else:
        acc_ref, m_ref, l_ref = take(3)
    lat_ref, kc_ref, vt_ref, sems = take(4)

    copies = []

    def bring(r, to):
        copies.append(pltpu.make_async_copy(r, to, sems.at[len(copies)]))
        copies[-1].start()

    if first:
        at = 0
        for r in q_refs:
            bring(r, queries_ref.at[at : at + r.shape[0]])
            at += r.shape[0]
    at = 0
    for r in pieces:
        bring(r, lat_ref.at[at : at + rows])
        at += rows

    if first:
        for copy in copies[:4]:
            copy.wait()
        qt = queries_ref[...].astype(f32).T
        cosine, sine = cos_ref[...], sin_ref[...]

        def rotated(at):
            a, b = qt[at : at + 32], qt[at + 32 : at + 64]
            return (a * cosine - b * sine).astype(bf16), (b * cosine + a * sine).astype(bf16)

        zeros = jnp.zeros((64, nq), bf16)
        for h in range(4):
            if h < 2:
                at = h * (DB + ROPE)
                qt_ref[h, 0:128] = qt[at : at + DB].astype(bf16)
                one, two = rotated(at + DB)
            else:
                at = 2 * (DB + ROPE) + (h - 2) * (DN + ROPE)
                used, others = (h - 2) * 64, (3 - h) * 64
                qt_ref[h, used : used + 64] = qt[at : at + DN].astype(bf16)
                qt_ref[h, others : others + 64] = zeros
                one, two = rotated(at + DN)
            qt_ref[h, 128:160] = one
            qt_ref[h, 160:192] = two
            qt_ref[h, 192:256] = zeros
        acc_ref[...] = jnp.zeros_like(acc_ref)
        l_ref[...] = jnp.zeros_like(l_ref)
        m_ref[...] = jnp.full_like(m_ref, low)
        for copy in copies[4:]:
            copy.wait()
    else:
        acc_ref[...] = acc_in[...]
        m_ref[...] = m_in[...]
        l_ref[...] = l_in[...]
        for copy in copies:
            copy.wait()

    def step(at, seen):
        chunk = lat_ref[pl.ds(at, nk), :]
        normed, rope = chunk[:, :R], chunk[:, R:]
        keys = jnp.dot(normed, wk_ref[...], preferred_element_type=f32).astype(bf16)
        for k in range(3):
            kc_ref[k, :, 0:128] = keys[:, 128 * k : 128 * (k + 1)]
            kc_ref[k, :, 128:256] = rope
        vt_ref[...] = lax.dot_general(
            wvt_ref[...], normed, (((1,), (1,)), ((), ())), preferred_element_type=f32
        ).astype(bf16)
        hide = jnp.where(seen, 0.0, low)
        keep = jnp.where(seen, 1.0, 0.0)
        if first:
            row = lax.broadcasted_iota(jnp.int32, (half, 1), 0)
            side = (row >= rows).astype(jnp.int32)
            core = c + side * (1 - 2 * c)
            key_pos = ((z * NY + y) * NC + core) * rows + row - side * rows

        def q_tile(t, carry):
            lanes = pl.ds(pl.multiple_of(t * tile, tile), tile)
            if first:
                col = lax.broadcasted_iota(jnp.int32, (1, tile), 1) + t * tile
                block = (col >= rows).astype(jnp.int32)
                block += (col >= 2 * rows).astype(jnp.int32)
                block += (col >= 3 * rows).astype(jnp.int32)
                yq = y - block
                yq = jnp.where(yq < 0, yq + NY, yq)
                q_pos = ((z * NY + yq) * NC + c) * rows + col - block * rows
                allowed = key_pos <= q_pos

            def scores(h):
                return jnp.dot(
                    kc_ref[min(h, 2)], qt_ref[h, :, lanes], preferred_element_type=f32
                )

            ahead = scores(0)
            for h in range(4):
                scale = LOG2E * ((DB if h < 2 else DN) + ROPE) ** (-0.5)
                s0, s1 = ahead[:half], ahead[half:]
                if h < 3:
                    ahead = scores(h + 1)
                if first:
                    s0 = jnp.where(allowed, s0, low)
                s1 = s1 + hide
                old = m_ref[h : h + 1, lanes]
                new = jnp.maximum(
                    jnp.maximum(old, jnp.max(s0, axis=0, keepdims=True)),
                    jnp.max(s1, axis=0, keepdims=True),
                )
                w0 = jnp.exp2((s0 - new) * scale)
                w1 = jnp.exp2((s1 - new) * scale)
                if first:
                    w0 = jnp.where(allowed, w0, 0.0)
                    w1 = w1 * keep
                factor = jnp.exp2((old - new) * scale)
                m_ref[h : h + 1, lanes] = new
                l_ref[h : h + 1, lanes] = (
                    l_ref[h : h + 1, lanes] * factor
                    + jnp.sum(w0, axis=0, keepdims=True)
                    + jnp.sum(w1, axis=0, keepdims=True)
                )
                dims = slice(h * 128, h * 128 + 128) if h < 2 else slice(128 + h * 64, 192 + h * 64)
                weight = jnp.concatenate([w0.astype(bf16), w1.astype(bf16)], axis=0)
                acc_ref[dims, lanes] = acc_ref[dims, lanes] * factor + jnp.dot(
                    vt_ref[dims, :], weight, preferred_element_type=f32
                )
            return carry

        lax.fori_loop(0, nq // tile, q_tile, 0)

    if first:
        step(0, z >= 1)
    else:

        def one_pair(i, carry):
            dmin, dmax = reach[0] + i, reach[1] - i

            @pl.when(dmin <= z)
            def _():
                step(pl.multiple_of(i * nk, nk), dmax <= z)

            return carry

        lax.fori_loop(0, len(pieces) // 4, one_pair, 0)

    if last:
        total = l_ref[...]
        some = total > 0.0
        safe = jnp.where(some, total, 1.0)
        inverse = jnp.where(some, 1.0 / safe, 0.0)
        head = lax.broadcasted_iota(jnp.int32, (8, 1), 0)
        scale = jnp.where(head < 2, LOG2E * (DB + ROPE) ** (-0.5), LOG2E * (DN + ROPE) ** (-0.5))
        lse = jnp.where(some, m_ref[...] * scale + jnp.log2(safe), low)
        high = lse.astype(bf16).astype(f32)
        middle = (lse - high).astype(bf16).astype(f32)
        parts = [
            acc_ref[0:128] * inverse[0:1],
            acc_ref[128:256] * inverse[1:2],
            acc_ref[256:320] * inverse[2:3],
            acc_ref[320:384] * inverse[3:4],
        ]
        packed = jnp.concatenate(parts, axis=0).T.astype(bf16)
        tail = lse - high - middle
        for e in range(NY):
            yq = y - e
            yq = jnp.where(yq < 0, yq + NY, yq)
            span = slice(e * rows, (e + 1) * rows)
            above = jnp.concatenate([high[0:4, span], middle[0:4, span]], axis=1)
            below = jnp.concatenate([tail[0:4, span], jnp.zeros((4, rows), f32)], axis=1)
            out_ref[yq, 0:rows] = packed[span]
            out_ref[yq, rows : rows + 8] = jnp.concatenate([above, below], axis=0).astype(bf16)


def attend(where, start, blocks, wk, wvt, rows, first=False, last=False, reach=(0, 1), limit=30):
    nq, nk = NY * rows, 4 * rows
    f32, bf16 = jnp.float32, jnp.bfloat16
    vmem = pl.BlockSpec(memory_space=pltpu.VMEM)
    hbm = pl.BlockSpec(memory_space=pltpu.HBM)
    pieces = blocks
    state = [((384, nq), f32), ((8, nq), f32), ((8, nq), f32)]
    queries = ((4, 256, nq), bf16)
    scratch = []
    if first:
        out = [queries] + state
        scratch.append(pltpu.VMEM((nq, 640), bf16))
        specs = [hbm] * 4 + [vmem] * 2
    elif last:
        out = [((NY, rows + 8, 2 * rows), bf16)]
        scratch += [pltpu.VMEM(*s) for s in state]
        specs = [vmem] * 4
    else:
        out = state
        specs = [vmem] * 4
    pairs = len(blocks) // 4
    scratch += [
        pltpu.VMEM((pairs * nk, 640), bf16),
        pltpu.VMEM((3, nk, 256), bf16),
        pltpu.VMEM((384, nk), bf16),
        pltpu.SemaphoreType.DMA((len(pieces) + 4 * first,)),
    ]
    result = pl.pallas_call(
        functools.partial(attend_kernel, rows=rows, first=first, last=last, reach=reach),
        out_shape=tuple(jax.ShapeDtypeStruct(*s) for s in out),
        in_specs=[pl.BlockSpec(memory_space=pltpu.SMEM)]
        + specs
        + [hbm] * len(pieces)
        + [vmem] * 2,
        out_specs=tuple(vmem for _ in out),
        scratch_shapes=scratch,
        compiler_params=pltpu.CompilerParams(
            vmem_limit_bytes=limit * 1024 * 1024
        ),
        cost_estimate=pl.CostEstimate(
            flops=pairs * 6_000_000_000, bytes_accessed=pairs * 2_000_000, transcendentals=3_000_000
        ),
        name="attend_last" if last else "attend_first" if first else "attend_next",
    )(where, *start, *pieces, wk, wvt)
    return result


def combine_kernel(part_ref, out_ref):
    f32 = jnp.float32
    rows = out_ref.shape[0]
    stats = []
    for s in range(NY):
        st = part_ref[s, rows : rows + 8, :].astype(f32)
        stats.append(st[0:4, :rows] + st[0:4, rows:] + st[4:8, :rows])
    top = functools.reduce(jnp.maximum, stats)
    weights = [jnp.exp2(st - top) for st in stats]
    inverse = 1.0 / functools.reduce(jnp.add, weights)
    table = jnp.concatenate([w * inverse for w in weights] * 2, axis=0).T
    lane = lax.broadcasted_iota(jnp.int32, (1, 128), 1)
    for k in range(3):
        total = None
        for s in range(NY):
            at = 4 * s
            if k < 2:
                factor = table[:, at + k : at + k + 1]
            else:
                factor = jnp.where(lane < 64, table[:, at + 2 : at + 3], table[:, at + 3 : at + 4])
            term = part_ref[s, 0:rows, 128 * k : 128 * (k + 1)].astype(f32) * factor
            total = term if total is None else total + term
        out_ref[:, 128 * k : 128 * (k + 1)] = total.astype(jnp.bfloat16)


def combine(parts):
    vmem = pl.BlockSpec(memory_space=pltpu.VMEM)
    return pl.pallas_call(
        combine_kernel,
        out_shape=jax.ShapeDtypeStruct((parts.shape[1] - 8, 384), jnp.bfloat16),
        in_specs=[vmem],
        out_specs=vmem,
        compiler_params=pltpu.CompilerParams(vmem_limit_bytes=8 * 1024 * 1024),
        cost_estimate=pl.CostEstimate(flops=1_000_000, bytes_accessed=1_000_000, transcendentals=0),
        name="combine",
    )(parts)


def project_own_kernel(where_ref, own_ref, broad_ref, narrow_ref, sum_ref, rest_ref, mine_ref, sems):
    x = where_ref[0]
    copies = []
    for d in range(4):
        xd = x - d
        xd = jnp.where(xd < 0, xd + 4, xd)
        to = mine_ref if d == 0 else rest_ref.at[d - 1]
        for r, size, at in ((broad_ref, 256, 0), (narrow_ref, 128, 256)):
            rows = pl.ds(pl.multiple_of(xd * size, size), size)
            copies.append(
                pltpu.make_async_copy(r.at[rows], to.at[at : at + size], sems.at[len(copies)])
            )
            copies[-1].start()
    for copy in copies[:2]:
        copy.wait()
    sum_ref[...] = jnp.dot(own_ref[...], mine_ref[...], preferred_element_type=jnp.float32)
    for copy in copies[2:]:
        copy.wait()


def project_own(where, own, out_broad, out_narrow):
    vmem = pl.BlockSpec(memory_space=pltpu.VMEM)
    hbm = pl.BlockSpec(memory_space=pltpu.HBM)
    rows, width = own.shape[0], out_broad.shape[1]
    return pl.pallas_call(
        project_own_kernel,
        out_shape=(
            jax.ShapeDtypeStruct((rows, width), jnp.float32),
            jax.ShapeDtypeStruct((3, 384, width), jnp.bfloat16),
        ),
        in_specs=[pl.BlockSpec(memory_space=pltpu.SMEM), vmem, hbm, hbm],
        out_specs=(vmem, vmem),
        scratch_shapes=[pltpu.VMEM((384, width), jnp.bfloat16), pltpu.SemaphoreType.DMA((8,))],
        compiler_params=pltpu.CompilerParams(vmem_limit_bytes=20 * 1024 * 1024),
        cost_estimate=pl.CostEstimate(
            flops=2_000_000_000, bytes_accessed=8_000_000, transcendentals=0
        ),
        name="project_own",
    )(where, own, out_broad, out_narrow)


def project_kernel(
    p1_ref, p2_ref, p3_ref, sum_ref, rest_ref, resid_ref, post_ref, gain_ref, mixed_ref, normed_ref
):
    f32, bf16 = jnp.float32, jnp.bfloat16
    projected = sum_ref[...] + jnp.dot(
        jnp.concatenate([p1_ref[...], p2_ref[...], p3_ref[...]], axis=1),
        jnp.concatenate([rest_ref[0], rest_ref[1], rest_ref[2]], axis=0),
        preferred_element_type=f32,
    )
    mixed = (resid_ref[...].astype(f32) + rms_scale(projected, post_ref[...])).astype(bf16)
    mixed_ref[...] = mixed
    normed_ref[...] = rms_scale(mixed.astype(f32), gain_ref[...]).astype(bf16)


def project(pieces, own_sum, rest, resid, post_gain, ffn_gain):
    vmem = pl.BlockSpec(memory_space=pltpu.VMEM)
    rows, width = resid.shape
    shape = jax.ShapeDtypeStruct((rows, width), jnp.bfloat16)
    return pl.pallas_call(
        project_kernel,
        out_shape=(shape, shape),
        in_specs=[vmem] * 8,
        out_specs=(vmem, vmem),
        compiler_params=pltpu.CompilerParams(vmem_limit_bytes=20 * 1024 * 1024),
        cost_estimate=pl.CostEstimate(
            flops=2 * rows * 1152 * width, bytes_accessed=8_000_000, transcendentals=0
        ),
        name="project",
    )(*pieces, own_sum, rest, resid, post_gain[None], ffn_gain[None])


def ffn_kernel(where_ref, *refs, tile, first):
    f32, bf16 = jnp.float32, jnp.bfloat16
    if first:
        normed_ref, both_ref, *out_refs = refs[:6]
        hidden_ref, up_ref, down_ref, sum_ref, up_sem, down_sem = refs[6:]
    else:
        hidden_ref, both_ref, *out_refs = refs[:6]
        down_ref, sum_ref, down_sem = refs[6:]
    units = hidden_ref.shape[1]
    width = both_ref.shape[0]
    steps, parts = units // tile, width // tile // 2
    skipped = 0 if first else parts

    def down_copy(i):
        at = pl.ds(pl.multiple_of((i + skipped) * tile, tile), tile)
        to = pl.ds(pl.multiple_of(i * tile, tile), tile)
        return pltpu.make_async_copy(
            both_ref.at[at, pl.ds(units, units)], down_ref.at[to, :], down_sem.at[i]
        )

    if first:

        def up_copy(i):
            at = pl.ds(pl.multiple_of(i * tile, tile), tile)
            return pltpu.make_async_copy(both_ref.at[:, at], up_ref.at[:, at], up_sem.at[i])

        for i in range(steps):
            up_copy(i).start()

        def hide(i, carry):
            at = pl.ds(pl.multiple_of(i * tile, tile), tile)
            up_copy(i).wait()

            @pl.when(i < parts)
            def _():
                down_copy(i).start()

            up = jnp.dot(normed_ref[...], up_ref[:, at], preferred_element_type=f32)
            hidden_ref[:, at] = jnp.square(jnp.maximum(up, 0.0)).astype(bf16)
            return carry

        lax.fori_loop(0, steps, hide, 0)
    else:
        for i in range(parts):
            down_copy(i).start()

    def multiply(i, carry):
        at = pl.ds(pl.multiple_of(i * tile, tile), tile)
        down_copy(i).wait()
        term = lax.dot_general(
            hidden_ref[...], down_ref[at, :], (((1,), (1,)), ((), ())), preferred_element_type=f32
        )
        sum_ref[:, at] = term.astype(bf16)
        return carry

    lax.fori_loop(0, parts, multiply, 0)

    x = where_ref[0]
    rows = out_refs[0].shape[0]
    for d, out_ref in enumerate(out_refs):
        xd = x + d
        xd = jnp.where(xd >= 4, xd - 4, xd)
        out_ref[...] = sum_ref[pl.ds(pl.multiple_of(xd * rows, rows), rows), :]


def feed_forward(where, operand, both, units, first):
    rows, width = operand.shape[0], both.shape[0]
    tile, bf16 = 512, jnp.bfloat16
    vmem = pl.BlockSpec(memory_space=pltpu.VMEM)
    half = width // 2
    out = [jax.ShapeDtypeStruct((rows // 4, half), bf16)] * 4
    scratch = [
        pltpu.VMEM((half, units), bf16),
        pltpu.VMEM((rows, half), bf16),
        pltpu.SemaphoreType.DMA((half // tile,)),
    ]
    if first:
        out.append(jax.ShapeDtypeStruct((rows, units), bf16))
        up_sem = pltpu.SemaphoreType.DMA((units // tile,))
        scratch = [pltpu.VMEM((width, units), bf16), *scratch[:2], up_sem, scratch[2]]
    return pl.pallas_call(
        functools.partial(ffn_kernel, tile=tile, first=first),
        out_shape=tuple(out),
        in_specs=[
            pl.BlockSpec(memory_space=pltpu.SMEM),
            vmem,
            pl.BlockSpec(memory_space=pltpu.HBM),
        ],
        out_specs=tuple(vmem for _ in out),
        scratch_shapes=scratch,
        compiler_params=pltpu.CompilerParams(vmem_limit_bytes=50 * 1024 * 1024),
        cost_estimate=pl.CostEstimate(
            flops=2_000_000_000, bytes_accessed=4 * width * units, transcendentals=0
        ),
        name="feed_forward_first" if first else "feed_forward_second",
    )(where, operand, both)


def angles(positions):
    frequency = rope_base ** (-2.0 * jnp.arange(ROPE // 2, dtype=jnp.float32) / ROPE)
    return positions.astype(jnp.float32), frequency


def local(
    resid, query_broad, query_narrow, latent, key_rope, latent_gain, key_up_broad, value_up_broad,
    key_up_narrow, value_up_narrow, out_broad, out_narrow, post_gain, ffn_gain, up_weight,
    down_weight, ffn_out_gain,
):
    f32, bf16 = jnp.float32, jnp.bfloat16
    rows = resid.shape[0]
    z, y, c = (lax.axis_index(a) for a in SP)
    first = ((z * NY + y) * NC + c) * rows
    within = jnp.arange(rows, dtype=jnp.int32)

    both = lax.all_gather(
        jnp.concatenate([up_weight, down_weight], axis=1), SP, axis=0, tiled=True
    )

    normed_latent = rms_scale(latent.astype(f32), latent_gain).astype(bf16)
    pos, frequency = angles(first + within)
    angle = pos[:, None] * frequency[None, :]
    ka, kb = key_rope[:, :32].astype(f32), key_rope[:, 32:].astype(f32)
    cosine, sine = jnp.cos(angle), jnp.sin(angle)
    key_rot = jnp.concatenate([ka * cosine - kb * sine, kb * cosine + ka * sine], axis=1)
    sent = jnp.concatenate(
        [normed_latent, key_rot.astype(bf16), jnp.zeros((rows, 64), bf16)], axis=1
    )
    block_y = jnp.mod(y - jnp.arange(NY, dtype=jnp.int32), NY)
    q_pos = ((z * NY + block_y) * NC + c)[:, None] * rows + within[None, :]
    pos, frequency = angles(q_pos.reshape(-1))
    angle = frequency[:, None] * pos[None, :]
    wk = jnp.concatenate([key_up_broad, key_up_narrow], axis=1)
    wvt = jnp.concatenate([value_up_broad, value_up_narrow], axis=1).T
    where = jnp.stack([z, y, c]).astype(jnp.int32)
    queries = jnp.concatenate([query_broad, query_narrow], axis=1)
    partial = attention(where, sent, queries, wk, wvt, jnp.cos(angle), jnp.sin(angle))
    parts = lax.all_to_all(partial, "y", 0, 0, tiled=True)
    attn = combine(parts)
    pieces = [shift(attn, "x", d) for d in (1, 2, 3)]
    nx, x = lax.axis_size("x"), lax.axis_index("x")
    place = x[None].astype(jnp.int32)
    own_sum, rest = project_own(place, attn, out_broad, out_narrow)
    mixed, normed = project(pieces, own_sum, rest, resid, post_gain, ffn_gain)
    units = up_weight.shape[1]
    *first, hidden = feed_forward(place, normed, both, units, True)
    sums = []
    come = [shift(first[d], "x", d) for d in (1, 2, 3)]
    second = feed_forward(place, hidden, both, units, False)
    for own, others in ((first[0], come), (second[0], None)):
        if others is None:
            others = [shift(second[d], "x", d) for d in (1, 2, 3)]
        sums.append(sum([o.astype(f32) for o in others], own.astype(f32)))
    ffn = jnp.concatenate(sums, axis=1)
    own_rows = rows // nx
    own = lax.dynamic_slice_in_dim(mixed, x * own_rows, own_rows, 0)
    return (own.astype(f32) + rms_scale(ffn, ffn_out_gain)).astype(bf16)


def solution(mesh):
    grid = Mesh(mesh.devices.reshape(NZ, NY, NC, -1), ("z", "y", "c", "x"))
    row, split, heads = P(SP, None), P(SP, "x"), P(None, "x")
    in_specs = (
        row, split, split, row, row, P(), heads, heads, heads, heads, P(), P(), P(), P(),
        split, split, P(),
    )
    return jax.shard_map(
        local, mesh=grid, in_specs=in_specs, out_specs=P(("z", "y", "c", "x"), None), check_vma=False
    )
```
